256 devices in a mesh: ep: 128 (over z, y, x), tp: 2 (over core).
Axes of the slice: x: 4, y: 4, z: 8, core: 2. Of those that a mesh axis runs over, the one named last changes fastest.
Arguments:
- tokens: bfloat16 [2048, 2048], P('ep'), may hold values from -6 to 6
- lengths: int32 [2048], P('ep'), may hold values from 1 to 1024, as said below
- attn_gain: float32 [2048], replicated, may hold values from 0.1 to 1.9
- w_query: bfloat16 [2048, 1024], P(None, 'tp'), may hold values from -0.125 to 0.125
- w_key: bfloat16 [2048, 128], P(None, 'tp'), may hold values from -0.125 to 0.125
- w_value: bfloat16 [2048, 128], P(None, 'tp'), may hold values from -0.125 to 0.125
- head_bias: float32 [16], P('tp'), may hold values from -7 to -2
- key_cache: bfloat16 [2048, 2, 64, 1024], P('ep', 'tp'), may hold values from -6 to 6
- value_cache: bfloat16 [2048, 2, 64, 1024], P('ep', 'tp'), may hold values from -6 to 6
- w_attn_out: bfloat16 [1024, 2048], P('tp'), may hold values from -0.1875 to 0.1875
- ffn_gain: float32 [2048], replicated, may hold values from 0.1 to 1.9
- w_router: bfloat16 [2048, 128], replicated, may hold values from -0.125 to 0.125
- routes: int32 [2048, 6], P('ep'), may hold values from 0 to 127, all different within a row; in each aligned block of 16 rows (0 to 15, 16 to 31, ...) at most 2 rows name the same one
- w_dense_gate: bfloat16 [2048, 512], P('ep', 'tp'), may hold values from -0.125 to 0.125
- w_dense_up: bfloat16 [2048, 512], P('ep', 'tp'), may hold values from -0.125 to 0.125
- w_dense_down: bfloat16 [512, 2048], P('tp', 'ep'), may hold values from -0.25 to 0.25
- dense_mix: float32 [2048], replicated, may hold values from -0.125 to 0.125
- w_expert_gate: bfloat16 [128, 2048, 512], P('ep', None, 'tp'), may hold values from -0.125 to 0.125
- w_expert_up: bfloat16 [128, 2048, 512], P('ep', None, 'tp'), may hold values from -0.125 to 0.125
- w_expert_down: bfloat16 [128, 512, 2048], P('ep', 'tp'), may hold values from -0.25 to 0.25
Outputs:
- layer_out: bfloat16 [2048, 2048], P('ep', 'tp')
- new_keys: bfloat16 [2048, 128], P('ep', 'tp')
- new_values: bfloat16 [2048, 128], P('ep', 'tp')
The draws below stay inside these ranges and needn't reach their ends.
Inputs may be any that keep to these rules, and one draw needn't show every extreme that they name: `lengths`: every sequence holds between 1 and 1024 cached positions; in every draw some sequence holds exactly 1024. `routes`: each token names 6 different experts. Among the rows of one device no expert is named by more than 2 rows.
All inputs are finite; a program needn't handle non-finite values.
Results may differ from the reference program's by a relative error of at most 0.014.
Values may be sent and summed in bfloat16 or wider, within the bound.
No kernel may reach another device: no remote copies, remote signals or barrier semaphores. Data moves between devices by JAX's collectives and lax.ppermute only.
A program may use at most 64 MiB of HBM per device.

```python
import math
import jax
import jax.numpy as jnp
import numpy as np
from jax import lax

D = 2048
HEADS = 16
KV_HEADS = 2
HEAD = 64
EXPERT_WIDTH = 512
SHARED = 512
TOP_K = 6
SEQ_DEV = 16
CACHE = 1024
EXPERTS = 128
TOKENS = 2048
CAP = 2
N_EP = 128
N_TP = 2


def draw_lengths(key, part):
    key_caps = jax.random.fold_in(key, 11)
    key_rows = jax.random.fold_in(key, 12)
    key_full = jax.random.fold_in(key, 13)
    group_total = TOKENS // SEQ_DEV
    device_caps = jax.random.randint(key_caps, (group_total, 1), CACHE // 8, CACHE + 1)
    drawn = jax.random.randint(key_rows, (group_total, SEQ_DEV), 1, device_caps + 1).reshape(-1)
    full_at = jax.random.randint(key_full, (), 0, TOKENS)
    drawn = jnp.where(jnp.arange(TOKENS, dtype=jnp.int32) == full_at, CACHE, drawn)
    return drawn.astype(jnp.int32)


def levels(rng, shape, pieces, least, top_value):
    level, own = 1.0, jax.random.fold_in(rng, 6)
    for position, shards_of in pieces:
        steps = jnp.exp(jax.random.uniform(jax.random.fold_in(own, position), (shards_of,), jnp.float32, least / len(pieces), top_value / len(pieces)))
        level = level * jnp.repeat(steps, shape[position] // shards_of).reshape([-1 if axis == position else 1 for axis in range(len(shape))])
    return level


def shared_out(own_key, own, number, rows, number_of, top, limit, slope):
    order = jax.random.permutation(own_key, number_of)
    crowded, ordinary = shares(number_of, rows * top, limit, slope, True), shares(number_of, rows * top, limit, slope, False)
    places = jnp.arange(number_of)

    def named(sizes, rotation):
        used = int((sizes > 0).sum())
        fixed = max(1, used // 4)
        shifted = fixed + (places - fixed + rotation * (used - fixed)) % max(1, number_of - fixed)
        return jnp.zeros((number_of,), jnp.int32).at[order[jnp.where(places < fixed, places, shifted)]].set(jnp.asarray(sizes, jnp.int32))

    sizes = jnp.where(number % 4 == 0, named(crowded, number // 4), named(ordinary, number - number // 4 - 1))
    mixed = jax.random.permutation(jax.random.fold_in(own, 3), number_of)
    donor, taker = mixed[0:number_of // 2 * 2:2], mixed[1:number_of // 2 * 2:2]
    margin = jnp.minimum(sizes[donor] - 1, limit - sizes[taker]) // 2
    margin = jnp.where((donor == order[0]) | (taker == order[0]) | (sizes[taker] == 0), 0, jnp.maximum(margin, 0))
    shifted = jax.random.randint(jax.random.fold_in(own, 4), (number_of // 2,), 0, 1 << 20) % (margin + 1)
    sizes = sizes.at[donor].add(-shifted).at[taker].add(shifted)
    members = jnp.searchsorted(jnp.cumsum(sizes), jnp.arange(rows * top), side="right").astype(jnp.int32)
    listing = members.reshape(top, rows).T
    listing = listing[jax.random.permutation(jax.random.fold_in(own, 1), rows)]
    rotation = jax.random.randint(jax.random.fold_in(own, 2), (rows, 1), 0, top)
    return jnp.take_along_axis(listing, (jnp.arange(top)[None, :] + rotation) % top, axis=1)


def shares(number_of, total, most, skew, full):
    loads = [(1 << 20) // math.isqrt(standing ** skew) + 1 for standing in range(1, number_of + 1)]
    largest = most if full else min(most, max(-(-total // number_of), total * loads[0] // sum(loads)))
    least = 1 if total - largest >= number_of - 1 else 0
    given, rest = [largest] + [least] * (number_of - 1), total - largest - least * (number_of - 1)
    while rest > 0:
        free = [i for i in range(1, number_of) if given[i] < largest] or [i for i in range(1, number_of) if given[i] < most]
        mass, budget = sum([loads[i] for i in free]), rest
        for i in free:
            addition = min(most - given[i], max(1, budget * loads[i] // mass), rest)
            given[i] = given[i] + addition
            rest = rest - addition
    return np.array(given)


def gaussian(own_key, extent, spread, most, split=(), held_as=jnp.bfloat16):
    level = levels(own_key, extent, split, -0.22, 0.18) if split else 1.0
    entries = jax.random.normal(own_key, extent, jnp.float32) * spread * level
    return jnp.minimum(jnp.maximum(entries, -most), most).astype(held_as)


def setup_inputs(seed: int = 0) -> dict:
    streams_of = jax.random.split(jax.random.key(seed), 21)
    tokens = gaussian(streams_of[0], (TOKENS, D), 1.0, 6.0, ((0, 128),))
    lengths = draw_lengths(jax.random.fold_in(streams_of[20], 71), 0)
    attn_gain = jnp.clip(1.0 + 0.18 * jax.random.normal(streams_of[2], (D,), jnp.float32), 0.1, 1.9)
    w_query = gaussian(streams_of[3], (D, HEADS * HEAD), D ** -0.5, 0.125, ((1, 2),))
    w_key = gaussian(streams_of[4], (D, KV_HEADS * HEAD), D ** -0.5, 0.125, ((1, 2),))
    w_value = gaussian(streams_of[5], (D, KV_HEADS * HEAD), D ** -0.5, 0.125, ((1, 2),))
    head_bias = jnp.clip(-7.0 + 5.0 * jax.random.uniform(streams_of[6], (HEADS,), jnp.float32) ** levels(streams_of[6], (HEADS,), ((0, 2),), -0.2, 0.2), -7.0, -2.0)
    key_cache = gaussian(streams_of[7], (TOKENS, KV_HEADS, HEAD, CACHE), 1.0, 6.0, ((0, 128), (1, 2)))
    value_cache = gaussian(streams_of[8], (TOKENS, KV_HEADS, HEAD, CACHE), 1.0, 6.0, ((0, 128), (1, 2)))
    w_attn_out = gaussian(streams_of[9], (HEADS * HEAD, D), (HEADS * HEAD) ** -0.5, 0.1875, ((0, 2),))
    ffn_gain = jnp.clip(1.0 + 0.18 * jax.random.normal(streams_of[10], (D,), jnp.float32), 0.1, 1.9)
    w_router = gaussian(streams_of[11], (D, EXPERTS), D ** -0.5, 0.125)
    routes_keys = jax.random.split(jax.random.fold_in(streams_of[12], 1), TOKENS // SEQ_DEV)
    routes_turns = jax.random.permutation(jax.random.fold_in(streams_of[12], 3), TOKENS // SEQ_DEV)
    routes = jax.vmap(lambda own, number: shared_out(jax.random.fold_in(streams_of[12], 2), own, number, SEQ_DEV, EXPERTS, TOP_K, CAP, 2))(routes_keys, routes_turns).reshape((TOKENS, TOP_K))
    w_dense_gate = gaussian(streams_of[13], (D, SHARED), D ** -0.5, 0.125, ((0, 128), (1, 2)))
    w_dense_up = gaussian(streams_of[14], (D, SHARED), D ** -0.5, 0.125, ((0, 128), (1, 2)))
    w_dense_down = gaussian(streams_of[15], (SHARED, D), SHARED ** -0.5, 0.25, ((0, 2), (1, 128)))
    dense_mix = gaussian(streams_of[16], (D,), D ** -0.5, 0.125, (), jnp.float32)
    w_expert_gate = gaussian(streams_of[17], (EXPERTS, D, EXPERT_WIDTH), D ** -0.5, 0.125, ((0, 128), (2, 2)))
    w_expert_up = gaussian(streams_of[18], (EXPERTS, D, EXPERT_WIDTH), D ** -0.5, 0.125, ((0, 128), (2, 2)))
    w_expert_down = gaussian(streams_of[19], (EXPERTS, EXPERT_WIDTH, D), EXPERT_WIDTH ** -0.5, 0.25, ((0, 128), (1, 2)))
    return {"tokens": tokens, "lengths": lengths, "attn_gain": attn_gain, "w_query": w_query, "w_key": w_key, "w_value": w_value, "head_bias": head_bias, "key_cache": key_cache, "value_cache": value_cache, "w_attn_out": w_attn_out, "ffn_gain": ffn_gain, "w_router": w_router, "routes": routes, "w_dense_gate": w_dense_gate, "w_dense_up": w_dense_up, "w_dense_down": w_dense_down, "dense_mix": dense_mix, "w_expert_gate": w_expert_gate, "w_expert_up": w_expert_up, "w_expert_down": w_expert_down}


def rms_scale(values, gain):
    wide = values.astype(jnp.float32)
    return wide * lax.rsqrt(lax.optimization_barrier(jnp.mean(wide * wide, axis=-1, keepdims=True)) + 1e-06) * gain

def halves_sum(hidden, down, rows):
    split_hidden = hidden.reshape(rows, N_TP, -1).astype(jnp.float32)
    split_down = down.reshape(N_TP, -1, D).astype(jnp.float32)
    parts = jnp.einsum('rnf,nfd->nrd', split_hidden, split_down).astype(jnp.bfloat16)
    return lax.optimization_barrier(jnp.sum(parts.astype(jnp.float32), axis=0))

def reference(tokens, lengths, attn_gain, w_query, w_key, w_value, head_bias, key_cache, value_cache, w_attn_out, ffn_gain, w_router, routes, w_dense_gate, w_dense_up, w_dense_down, dense_mix, w_expert_gate, w_expert_up, w_expert_down):
    normed = rms_scale(tokens, attn_gain).astype(jnp.bfloat16)
    queries = jnp.dot(normed, w_query, preferred_element_type=jnp.float32).astype(jnp.bfloat16)
    new_keys = jnp.dot(normed, w_key, preferred_element_type=jnp.float32).astype(jnp.bfloat16)
    new_values = jnp.dot(normed, w_value, preferred_element_type=jnp.float32).astype(jnp.bfloat16)
    group_size = HEADS // KV_HEADS
    block_total = TOKENS // SEQ_DEV
    grouped = queries.reshape(block_total, SEQ_DEV, KV_HEADS, group_size, HEAD)
    key_blocks = key_cache.reshape(block_total, SEQ_DEV, KV_HEADS, HEAD, CACHE)
    value_blocks = value_cache.reshape(block_total, SEQ_DEV, KV_HEADS, HEAD, CACHE)
    length_blocks = lengths.reshape(block_total, SEQ_DEV)
    head_shift = head_bias.reshape(1, KV_HEADS, group_size, 1)

    def attend(inputs):
        block_queries, block_keys, block_values, block_lengths = inputs
        scores = jnp.einsum('skgd,skdc->skgc', block_queries.astype(jnp.float32), block_keys.astype(jnp.float32)) * HEAD ** (-0.5) + head_shift
        visible = (jnp.arange(CACHE, dtype=jnp.int32)[None, :] < block_lengths[:, None])[:, None, None, :]
        log_keep = jnp.where(visible, jax.nn.log_sigmoid(-scores), 0.0)
        log_after = lax.cumsum(log_keep, axis=3, reverse=True) - log_keep
        weights = jnp.where(visible, jnp.exp(jax.nn.log_sigmoid(scores) + log_after), 0.0).astype(jnp.bfloat16)
        mixed = jnp.einsum('skgc,skdc->skgd', weights.astype(jnp.float32), block_values.astype(jnp.float32))
        return mixed.reshape(SEQ_DEV, HEADS * HEAD).astype(jnp.bfloat16)
    heads_out = lax.map(attend, (grouped, key_blocks, value_blocks, length_blocks)).reshape(TOKENS, HEADS * HEAD)
    attn = halves_sum(heads_out, w_attn_out, TOKENS)
    residual = (tokens.astype(jnp.float32) + attn).astype(jnp.bfloat16)
    normed2 = rms_scale(residual, ffn_gain).astype(jnp.bfloat16)
    probs = jax.nn.sigmoid(jnp.dot(normed2, w_router, preferred_element_type=jnp.float32))
    hits = routes[:, :, None] == jnp.arange(EXPERTS, dtype=jnp.int32)[None, None, :]
    picked = lax.optimization_barrier(jnp.sum(jnp.where(hits, probs[:, None, :], 0.0), axis=-1))
    gates = picked / lax.optimization_barrier(jnp.sum(picked, axis=-1, keepdims=True)) * 2.5
    flat_routes = routes.reshape(-1)
    route_total = TOKENS * TOP_K
    bound = N_EP * CAP
    padded_inputs = jnp.concatenate([normed2, jnp.zeros((1, D), jnp.bfloat16)], axis=0)

    def expert_pass(inputs):
        expert_id, gate_w, up_w, down_w = inputs
        chosen = jnp.nonzero(flat_routes == expert_id, size=bound, fill_value=route_total)[0].astype(jnp.int32)
        rows_in = padded_inputs[chosen // TOP_K]
        gate_rows = jnp.dot(rows_in, gate_w, preferred_element_type=jnp.float32)
        up_rows = jnp.dot(rows_in, up_w, preferred_element_type=jnp.float32)
        hidden = (jax.nn.silu(gate_rows) * up_rows).astype(jnp.bfloat16)
        return (halves_sum(hidden, down_w, bound).astype(jnp.bfloat16), chosen)
    expert_rows, chosen_all = lax.map(expert_pass, (jnp.arange(EXPERTS, dtype=jnp.int32), w_expert_gate, w_expert_up, w_expert_down))
    route_rows = jnp.zeros((route_total + 1, D), jnp.bfloat16).at[chosen_all.reshape(-1)].set(expert_rows.reshape(-1, D))[:route_total]
    routed = lax.optimization_barrier(jnp.sum(gates[:, :, None] * route_rows.reshape(TOKENS, TOP_K, D).astype(jnp.float32), axis=1))
    dense_gate_rows = jnp.dot(normed2, w_dense_gate, preferred_element_type=jnp.float32)
    dense_up_rows = jnp.dot(normed2, w_dense_up, preferred_element_type=jnp.float32)
    dense_hidden = (jax.nn.silu(dense_gate_rows) * dense_up_rows).astype(jnp.bfloat16)
    dense = halves_sum(dense_hidden, w_dense_down, TOKENS)
    mix_gate = jax.nn.sigmoid(lax.optimization_barrier(jnp.sum(normed2.astype(jnp.float32) * dense_mix, axis=-1)))
    layer_out = (residual.astype(jnp.float32) + mix_gate[:, None] * dense + routed).astype(jnp.bfloat16)
    return (layer_out, new_keys, new_values)
```

```python
import jax
import jax.numpy as jnp
from jax import lax
from jax.experimental import pallas as pl
from jax.experimental.pallas import tpu as pltpu
from jax.sharding import Mesh
from jax.sharding import PartitionSpec as P

EP = ("ep_0", "ep_1", "ep_2")
LINE = "ep_0"
PLANE = ("ep_1", "ep_2")
SWAP = ((0, 1), (1, 0))
F32 = jnp.float32
BF16 = jnp.bfloat16

GATE_HI, GATE_LO, MIX_HI, MIX_LO, DENSE = 8, 16, 24, 25, 32


def rms_scale(values, gain):
    wide = values.astype(F32)
    return wide * lax.rsqrt(jnp.mean(wide * wide, axis=-1, keepdims=True) + 1e-06) * gain


def stick_read(queries, lengths, head_bias, key_cache, value_cache):
    seq_count, local_kv, head_dim, cache_len = key_cache.shape
    group_size = head_bias.shape[0] // local_kv
    grouped = queries.reshape(seq_count, local_kv, group_size, head_dim)
    head_shift = head_bias.reshape(1, local_kv, group_size, 1)
    span_len = min(512, cache_len)
    block_count = (jnp.max(lengths) + span_len - 1) // span_len
    span_index = lax.iota(jnp.int32, span_len)
    after_mask = (span_index[:, None] > span_index[None, :]).astype(F32)

    def visit(visit_index, carry):
        totals, log_later = carry
        first = (block_count - 1 - visit_index) * span_len
        key_block = lax.dynamic_slice_in_dim(key_cache, first, span_len, 3)
        value_block = lax.dynamic_slice_in_dim(value_cache, first, span_len, 3)
        scores = (
            jnp.einsum("skgd,skdc->skgc", grouped, key_block, preferred_element_type=F32)
            * head_dim ** (-0.5)
            + head_shift
        )
        positions = first + span_index
        visible = (positions[None, :] < lengths[:, None])[:, None, None, :]
        log_keep = jnp.where(visible, jax.nn.log_sigmoid(-scores), 0.0)
        log_after = jnp.einsum("skgj,jc->skgc", log_keep, after_mask) + log_later[..., None]
        weights = jnp.where(visible, jnp.exp(jax.nn.log_sigmoid(scores) + log_after), 0.0).astype(
            BF16
        )
        totals = totals + jnp.einsum(
            "skgc,skdc->skgd", weights, value_block, preferred_element_type=F32
        )
        return (totals, log_later + jnp.sum(log_keep, axis=3))

    start_totals = jnp.zeros((seq_count, local_kv, group_size, head_dim), F32)
    start_later = jnp.zeros((seq_count, local_kv, group_size), F32)
    totals, unused_later = lax.fori_loop(0, block_count, visit, (start_totals, start_later))
    return totals.reshape(seq_count, -1).astype(BF16)


def call(kernel, out_shape, smem_count, inputs, limit=48):
    in_specs = [pl.BlockSpec(memory_space=pltpu.SMEM)] * smem_count
    in_specs += [pl.BlockSpec(memory_space=pltpu.VMEM)] * (len(inputs) - smem_count)
    return pl.pallas_call(
        kernel,
        out_shape=out_shape,
        in_specs=in_specs,
        out_specs=jax.tree.map(lambda _: pl.BlockSpec(memory_space=pltpu.VMEM), out_shape),
        compiler_params=pltpu.CompilerParams(vmem_limit_bytes=limit * 1024 * 1024),
    )(*inputs)


def rows_kernel(
    core_ref,
    tokens_ref,
    own_ref,
    other_ref,
    gain_ref,
    router_ref,
    routes_ref,
    gate_ref,
    up_ref,
    down_ref,
    mix_ref,
    send_ref,
    residual_ref,
):
    first_core = core_ref[0] == 0
    lines, seq_count, _ = send_ref.shape
    half = residual_ref.shape[1]
    attn = own_ref[...].astype(F32) + other_ref[...].astype(F32)
    residual = (tokens_ref[...].astype(F32) + attn).astype(BF16)
    normed = rms_scale(residual, gain_ref[...]).astype(BF16)
    residual_ref[...] = jnp.where(first_core, residual[:, :half], residual[:, half:])
    probs = jax.nn.sigmoid(jnp.dot(normed, router_ref[...], preferred_element_type=F32))
    mix = jax.nn.sigmoid(jnp.sum(normed.astype(F32) * mix_ref[...], axis=-1, keepdims=True))
    routes = routes_ref[...]
    lane = lax.broadcasted_iota(jnp.int32, probs.shape, 1)
    picked = [
        jnp.sum(jnp.where(lane == routes[:, k : k + 1], probs, 0.0), axis=-1, keepdims=True)
        for k in range(routes.shape[1])
    ]
    total = sum(picked[1:], picked[0])
    meta_lane = lax.broadcasted_iota(jnp.int32, (seq_count, 128), 1)
    meta = jnp.zeros((seq_count, 128), F32)

    def put(meta, at, value):
        return jnp.where(meta_lane == at, value, meta)

    for k, one in enumerate(picked):
        gate = one / total * 2.5
        high = gate.astype(BF16).astype(F32)
        meta = put(meta, k, routes[:, k : k + 1].astype(F32))
        meta = put(meta, GATE_HI + k, high)
        meta = put(meta, GATE_LO + k, gate - high)
    mix_high = mix.astype(BF16).astype(F32)
    meta = put(put(meta, MIX_HI, mix_high), MIX_LO, mix - mix_high)
    eye = (
        lax.broadcasted_iota(jnp.int32, (seq_count, seq_count), 0)
        == lax.broadcasted_iota(jnp.int32, (seq_count, seq_count), 1)
    ).astype(BF16)
    down = lax.dot_general(eye, down_ref[...], (((1,), (1,)), ((), ())), preferred_element_type=F32)
    parts = (gate_ref[...].astype(F32), up_ref[...].astype(F32), down)
    part = parts[0].shape[1] // lines
    row = jnp.where(first_core, normed[:, :half], normed[:, half:])
    for line in range(lines):
        block = meta
        at = line * part
        for n, values in enumerate(parts):
            tile = values[:, at // 128 * 128 : at // 128 * 128 + 128]
            to = DENSE + n * part
            moved = pltpu.roll(tile, (to - at % 128) % 128, 1)
            inside = jnp.logical_and(meta_lane >= to, meta_lane < to + part)
            block = jnp.where(inside, moved, block)
        send_ref[line, :, :half] = row
        send_ref[line, :, half:] = block.astype(BF16)


def slots_kernel(line_ref, got_ref, send_ref, combine_ref):
    lines, seq_count, width = got_ref.shape
    places, _, half = send_ref.shape
    token_total = lines * seq_count
    capacity = seq_count
    slot_total = places * capacity
    got = got_ref[...].reshape(token_total, width)
    meta = got[:, half:].astype(F32).T
    slot = lax.broadcasted_iota(jnp.int32, (slot_total, token_total), 0)
    token = lax.broadcasted_iota(jnp.int32, (slot_total, token_total), 1)
    expert = (line_ref[0] * places + slot // capacity).astype(F32)
    hit = jnp.zeros((slot_total, token_total), F32)
    gate = jnp.zeros((slot_total, token_total), F32)
    for k in range(6):
        same = meta[k : k + 1] == expert
        hit = jnp.where(same, 1.0, hit)
        gate = jnp.where(same, meta[GATE_HI + k : GATE_HI + k + 1] + meta[GATE_LO + k : GATE_LO + k + 1], gate)
    row = lax.broadcasted_iota(jnp.int32, (token_total, token_total), 0)
    column = lax.broadcasted_iota(jnp.int32, (token_total, token_total), 1)
    earlier = jnp.logical_and(row // seq_count == column // seq_count, row < column)
    rank = jnp.dot(hit.astype(BF16), earlier.astype(BF16), preferred_element_type=F32)
    per_source = capacity // lines
    here = jnp.logical_and(
        token // seq_count == slot % capacity // per_source,
        rank == (slot % per_source).astype(F32),
    )
    chosen = jnp.where(here, hit, 0.0)
    rows = jnp.dot(chosen.astype(BF16), got[:, :half], preferred_element_type=F32)
    send_ref[:, :capacity, :] = rows.astype(BF16).reshape(places, capacity, half)
    for line in range(lines):
        block = got_ref[line, :, half:]
        send_ref[:, capacity:, line * 128 : line * 128 + 128] = jnp.broadcast_to(
            block[None], (places, seq_count, 128)
        )
    weights = jnp.where(here, gate * hit, 0.0).T
    high = weights.astype(BF16)
    combine_ref[:, :slot_total] = high
    combine_ref[:, slot_total:] = (weights - high.astype(F32)).astype(BF16)


def experts_kernel(
    core_ref, own_ref, other_ref, line_own_ref, line_other_ref, gate_ref, up_ref, down_ref, keep_ref, send_ref
):
    core = core_ref[0]
    places, rows, half = own_ref.shape
    capacity = rows // 2
    slot_total = places * capacity
    lines, seq_count, _ = line_own_ref.shape
    token_total = lines * seq_count
    mine = pl.ds(pl.multiple_of(core * half, half), half)
    theirs = pl.ds(pl.multiple_of((1 - core) * half, half), half)
    x_own = own_ref[:, :capacity, :].reshape(slot_total, half)
    x_other = other_ref[:, :capacity, :].reshape(slot_total, half)

    def project(weight_ref):
        return jnp.dot(x_own, weight_ref[mine, :], preferred_element_type=F32) + jnp.dot(
            x_other, weight_ref[theirs, :], preferred_element_type=F32
        )

    hidden = (jax.nn.silu(project(gate_ref)) * project(up_ref)).astype(BF16)
    keep_ref[:slot_total, :] = jnp.dot(hidden, down_ref[:, mine], preferred_element_type=F32).astype(BF16)
    send_ref[:slot_total, :] = jnp.dot(hidden, down_ref[:, theirs], preferred_element_type=F32).astype(BF16)

    half_lines = lines // 2
    block = half // half_lines

    def dense_weights(line):
        at = pl.multiple_of(line * 128, 128)
        return own_ref[:, capacity:, pl.ds(at, 128)].reshape(block, 128)

    line_own = line_own_ref[:, :, :half].reshape(token_total, half)
    line_other = line_other_ref[:, :, :half].reshape(token_total, half)
    sums = jnp.zeros((token_total, 128), F32)
    for k in range(half_lines):
        at = slice(k * block, (k + 1) * block)
        sums += jnp.dot(line_own[:, at], dense_weights(core * half_lines + k), preferred_element_type=F32)
        sums += jnp.dot(line_other[:, at], dense_weights((1 - core) * half_lines + k), preferred_element_type=F32)
    lane = lax.broadcasted_iota(jnp.int32, sums.shape, 1)
    gate = pltpu.roll(sums, 64, 1)
    up = pltpu.roll(sums, 32, 1)
    dense = jnp.where(lane >= 96, jax.nn.silu(gate) * up, 0.0).astype(BF16)
    for k in range(half_lines):
        at = slice(k * block, (k + 1) * block)
        for target, side in ((keep_ref, core), (send_ref, 1 - core)):
            target[slot_total:, at] = lax.dot_general(
                dense,
                dense_weights(side * half_lines + k),
                (((1,), (1,)), ((), ())),
                preferred_element_type=F32,
            ).astype(BF16)


def combine_kernel(back_ref, combine_ref, line_ref, keep_ref, got_ref, send_ref):
    lines, seq_count, half = send_ref.shape
    token_total = lines * seq_count
    slot_total = back_ref.shape[0] * back_ref.shape[1]
    back = back_ref[...].reshape(slot_total, half)
    routed = jnp.dot(combine_ref[:, :slot_total], back, preferred_element_type=F32)
    routed += jnp.dot(combine_ref[:, slot_total:], back, preferred_element_type=F32)
    meta = line_ref[...].reshape(token_total, line_ref.shape[2])[:, half:].astype(F32)
    mix = meta[:, MIX_HI : MIX_HI + 1] + meta[:, MIX_LO : MIX_LO + 1]
    dense = keep_ref[slot_total:, :].astype(F32) + got_ref[slot_total:, :].astype(F32)
    send_ref[...] = (routed + mix * dense).astype(BF16).reshape(lines, seq_count, half)


def shards(
    tokens,
    lengths,
    attn_gain,
    w_query,
    w_key,
    w_value,
    head_bias,
    key_cache,
    value_cache,
    w_attn_out,
    ffn_gain,
    w_router,
    routes,
    w_dense_gate,
    w_dense_up,
    w_dense_down,
    dense_mix,
    w_expert_gate,
    w_expert_up,
    w_expert_down,
):
    seq_count, width = tokens.shape
    half = width // 2
    lines = lax.axis_size(LINE)
    places = lax.axis_size(PLANE)
    slot_total = places * seq_count
    token_total = lines * seq_count
    core = lax.axis_index("tp").astype(jnp.int32).reshape(1)
    line = lax.axis_index(LINE).astype(jnp.int32).reshape(1)
    normed = rms_scale(tokens, attn_gain).astype(BF16)
    new_keys = jnp.dot(normed, w_key, preferred_element_type=F32).astype(BF16)
    new_values = jnp.dot(normed, w_value, preferred_element_type=F32).astype(BF16)
    queries = jnp.dot(normed, w_query, preferred_element_type=F32).astype(BF16)
    heads_out = stick_read(queries, lengths, head_bias, key_cache, value_cache)
    attn_own = jnp.dot(heads_out, w_attn_out, preferred_element_type=F32).astype(BF16)
    attn_other = lax.ppermute(attn_own, "tp", SWAP)
    line_send, residual = call(
        rows_kernel,
        (
            jax.ShapeDtypeStruct((lines, seq_count, half + 128), BF16),
            jax.ShapeDtypeStruct((seq_count, half), BF16),
        ),
        1,
        (
            core,
            tokens,
            attn_own,
            attn_other,
            ffn_gain.reshape(1, width),
            w_router,
            routes,
            w_dense_gate,
            w_dense_up,
            w_dense_down,
            dense_mix.reshape(1, width),
        ),
    )
    line_own = lax.all_to_all(line_send, LINE, 0, 0, tiled=True)
    line_other = lax.ppermute(line_own, "tp", SWAP)
    slot_send, combine = call(
        slots_kernel,
        (
            jax.ShapeDtypeStruct((places, 2 * seq_count, half), BF16),
            jax.ShapeDtypeStruct((token_total, 2 * slot_total), BF16),
        ),
        1,
        (line, line_own),
    )
    slot_own = lax.all_to_all(slot_send, PLANE, 0, 0, tiled=True)
    slot_other = lax.ppermute(slot_own, "tp", SWAP)
    keep, send = call(
        experts_kernel,
        (jax.ShapeDtypeStruct((slot_total + token_total, half), BF16),) * 2,
        1,
        (
            core,
            slot_own,
            slot_other,
            line_own,
            line_other,
            w_expert_gate[0],
            w_expert_up[0],
            w_expert_down[0],
        ),
    )
    got = lax.ppermute(send, "tp", SWAP)
    results = (keep[:slot_total].astype(F32) + got[:slot_total].astype(F32)).astype(BF16)
    back = lax.all_to_all(results.reshape(places, seq_count, half), PLANE, 0, 0, tiled=True)
    partial = call(
        combine_kernel,
        jax.ShapeDtypeStruct((lines, seq_count, half), BF16),
        0,
        (back, combine, line_own, keep, got),
    )
    parts = lax.all_to_all(partial, LINE, 0, 0, tiled=True)
    layer_out = (residual.astype(F32) + jnp.sum(parts.astype(F32), axis=0)).astype(BF16)
    return (layer_out, new_keys, new_values)


def solution(mesh):
    finer = Mesh(mesh.devices.reshape(8, 4, 4, mesh.shape["tp"]), ("ep_0", "ep_1", "ep_2", "tp"))
    placed = (
        P(EP, None),
        P(EP),
        P(),
        P(None, "tp"),
        P(None, "tp"),
        P(None, "tp"),
        P("tp"),
        P(EP, "tp", None, None),
        P(EP, "tp", None, None),
        P("tp", None),
        P(),
        P(),
        P(EP, None),
        P(EP, "tp"),
        P(EP, "tp"),
        P("tp", EP),
        P(),
        P(EP, None, "tp"),
        P(EP, None, "tp"),
        P(EP, "tp", None),
    )
    return jax.shard_map(
        shards,
        mesh=finer,
        in_specs=placed,
        out_specs=(P(EP, "tp"), P(EP, "tp"), P(EP, "tp")),
        check_vma=False,
    )
```

```python
import jax
import jax.numpy as jnp
from jax import lax
from jax.experimental import pallas as pl
from jax.experimental.pallas import tpu as pltpu
from jax.sharding import Mesh
from jax.sharding import PartitionSpec as P

EP = ("ep_0", "ep_1", "ep_2")
LINE = "ep_0"
PLANE = ("ep_1", "ep_2")
SWAP = ((0, 1), (1, 0))
F32 = jnp.float32
BF16 = jnp.bfloat16

GATE_HI, GATE_LO, MIX_HI, MIX_LO, DENSE = 8, 16, 24, 25, 32


def rms_scale(values, gain):
    wide = values.astype(F32)
    return wide * lax.rsqrt(jnp.mean(wide * wide, axis=-1, keepdims=True) + 1e-06) * gain


def attend_kernel(
    bias_hbm,
    lengths_hbm,
    tokens_hbm,
    gain_hbm,
    query_hbm,
    key_hbm,
    value_hbm,
    out_hbm,
    partial_ref,
    bias_ref,
    lengths_ref,
    tokens_ref,
    gain_ref,
    query_buf,
    key_buf,
    value_buf,
    out_buf,
    sems,
):
    seq_count, width = tokens_ref.shape
    head_total = query_buf.shape[1]
    row_total, cache_len = key_buf.shape
    head_dim = row_total // seq_count
    heads = head_total // head_dim
    copies = []

    def fetch(source, target, pieces):
        size = source.shape[0] // pieces
        made = []
        for n in range(pieces):
            at = pl.ds(n * size, size)
            made.append(pltpu.make_async_copy(source.at[at, :], target.at[at, :], sems.at[len(copies)]))
            copies.append(made[-1])
        return made

    small_copies = [
        fetch(source, target, 1)[0]
        for source, target in (
            (tokens_hbm, tokens_ref),
            (gain_hbm, gain_ref),
            (bias_hbm, bias_ref),
            (lengths_hbm, lengths_ref),
        )
    ]
    query_copies = fetch(query_hbm, query_buf, 2)
    key_copies = fetch(key_hbm, key_buf, 2)
    value_copies = fetch(value_hbm, value_buf, 2)
    out_copies = fetch(out_hbm, out_buf, 1)
    for copy in copies:
        copy.start()

    for copy in small_copies:
        copy.wait()
    normed = rms_scale(tokens_ref[...], gain_ref[...]).astype(BF16)
    row = lax.broadcasted_iota(jnp.int32, (heads * seq_count, 1), 0)
    bias = jnp.zeros((heads * seq_count, 1), F32)
    for h in range(heads):
        bias = jnp.where(row // seq_count == h, bias_ref[:, h : h + 1], bias)
    lengths = jnp.zeros((seq_count, 1), jnp.int32)
    for n in range(seq_count):
        lengths = jnp.where(row[:seq_count] == n, lengths_ref[:, n : n + 1], lengths)
    lengths = jnp.concatenate([lengths] * heads, axis=0)
    lane = lax.broadcasted_iota(jnp.int32, (seq_count, 128), 1)
    low = lane < head_dim
    own = (
        lax.broadcasted_iota(jnp.int32, (seq_count, row_total), 1) // head_dim
        == lax.broadcasted_iota(jnp.int32, (seq_count, row_total), 0)
    )
    span = 256
    after_mask = (
        lax.broadcasted_iota(jnp.int32, (span, span), 0) > lax.broadcasted_iota(jnp.int32, (span, span), 1)
    ).astype(BF16)

    queries = jnp.zeros((seq_count, head_total), F32)
    piece = width // len(query_copies)
    for n, copy in enumerate(query_copies):
        copy.wait()
        at = slice(n * piece, (n + 1) * piece)
        queries += jnp.dot(normed[:, at], query_buf[at, :], preferred_element_type=F32)
    queries = queries.astype(BF16).astype(F32)
    spread = []
    for h in range(heads):
        tile = queries[:, h // 2 * 128 : h // 2 * 128 + 128]
        turned = pltpu.roll(tile, head_dim, 1)
        both = jnp.where(low, tile, turned) if h % 2 == 0 else jnp.where(low, turned, tile)
        wide = jnp.concatenate([both] * (row_total // 128), axis=1)
        spread.append(jnp.where(own, wide, 0.0).astype(BF16))
    spread = jnp.concatenate(spread, axis=0)

    scores = None
    piece = row_total // len(key_copies)
    for n, copy in enumerate(key_copies):
        copy.wait()
        at = slice(n * piece, (n + 1) * piece)
        part = jnp.dot(spread[:, at], key_buf[at, :], preferred_element_type=F32)
        scores = part if scores is None else scores + part
    later = jnp.zeros((heads * seq_count, 1), F32)
    sticks = []
    for block in reversed(range(cache_len // span)):
        score = scores[:, block * span : (block + 1) * span] * head_dim ** (-0.5) + bias
        position = lax.broadcasted_iota(jnp.int32, score.shape, 1) + block * span
        visible = position < lengths
        soft = jnp.log1p(jnp.exp(-jnp.abs(score)))
        log_keep = jnp.where(visible, -(jnp.maximum(score, 0.0) + soft), 0.0)
        high = log_keep.astype(BF16)
        rest = (log_keep - high.astype(F32)).astype(BF16)
        log_after = jnp.dot(high, after_mask, preferred_element_type=F32)
        log_after += jnp.dot(rest, after_mask, preferred_element_type=F32)
        weight = jnp.exp(jnp.minimum(score, 0.0) - soft + (log_after + later))
        sticks.append(jnp.where(visible, weight, 0.0).astype(BF16))
        later += jnp.sum(log_keep, axis=-1, keepdims=True)
    sticks = jnp.concatenate(sticks[::-1], axis=1)

    read = []
    piece = row_total // len(value_copies)
    for n, copy in enumerate(value_copies):
        copy.wait()
        read.append(
            lax.dot_general(
                sticks,
                value_buf[n * piece : (n + 1) * piece, :],
                (((1,), (1,)), ((), ())),
                preferred_element_type=F32,
            )
        )
    read = jnp.concatenate(read, axis=1)
    folded = []
    for h in range(heads):
        mine = jnp.where(own, read[h * seq_count : (h + 1) * seq_count], 0.0)
        tile = mine[:, :128]
        for n in range(1, row_total // 128):
            tile += mine[:, n * 128 : (n + 1) * 128]
        folded.append(tile + pltpu.roll(tile, head_dim, 1))
    heads_out = jnp.concatenate(
        [jnp.where(low, folded[h], folded[h + 1]) for h in range(0, heads, 2)], axis=1
    ).astype(BF16)
    for copy in out_copies:
        copy.wait()
    partial_ref[...] = jnp.dot(heads_out, out_buf[...], preferred_element_type=F32).astype(BF16)


def call(kernel, out_shape, smem_count, inputs, limit, hbm_count=0, scratch=()):
    in_specs = [pl.BlockSpec(memory_space=pltpu.SMEM)] * smem_count
    in_specs += [pl.BlockSpec(memory_space=pltpu.VMEM)] * (len(inputs) - smem_count - hbm_count)
    in_specs += [pl.BlockSpec(memory_space=pltpu.HBM)] * hbm_count
    return pl.pallas_call(
        kernel,
        out_shape=out_shape,
        in_specs=in_specs,
        out_specs=jax.tree.map(lambda _: pl.BlockSpec(memory_space=pltpu.VMEM), out_shape),
        scratch_shapes=scratch,
        compiler_params=pltpu.CompilerParams(vmem_limit_bytes=limit * 1024 * 1024),
    )(*inputs)


def rows_kernel(
    core_ref,
    tokens_ref,
    own_ref,
    other_ref,
    gain_ref,
    router_ref,
    routes_ref,
    gate_ref,
    up_ref,
    down_ref,
    mix_ref,
    send_ref,
    residual_ref,
):
    first_core = core_ref[0] == 0
    lines, seq_count, _ = send_ref.shape
    half = residual_ref.shape[1]
    attn = own_ref[...].astype(F32) + other_ref[...].astype(F32)
    residual = (tokens_ref[...].astype(F32) + attn).astype(BF16)
    normed = rms_scale(residual, gain_ref[...]).astype(BF16)
    residual_ref[...] = jnp.where(first_core, residual[:, :half], residual[:, half:])
    probs = jax.nn.sigmoid(jnp.dot(normed, router_ref[...], preferred_element_type=F32))
    mix = jax.nn.sigmoid(jnp.sum(normed.astype(F32) * mix_ref[...], axis=-1, keepdims=True))
    routes = routes_ref[...]
    lane = lax.broadcasted_iota(jnp.int32, probs.shape, 1)
    picked = [
        jnp.sum(jnp.where(lane == routes[:, k : k + 1], probs, 0.0), axis=-1, keepdims=True)
        for k in range(routes.shape[1])
    ]
    total = sum(picked[1:], picked[0])
    meta_lane = lax.broadcasted_iota(jnp.int32, (seq_count, 128), 1)
    meta = jnp.zeros((seq_count, 128), F32)

    def put(meta, at, value):
        return jnp.where(meta_lane == at, value, meta)

    for k, one in enumerate(picked):
        gate = one / total * 2.5
        high = gate.astype(BF16).astype(F32)
        meta = put(meta, k, routes[:, k : k + 1].astype(F32))
        meta = put(meta, GATE_HI + k, high)
        meta = put(meta, GATE_LO + k, gate - high)
    mix_high = mix.astype(BF16).astype(F32)
    meta = put(put(meta, MIX_HI, mix_high), MIX_LO, mix - mix_high)
    parts = [ref[...].astype(F32) for ref in (gate_ref, up_ref, down_ref)]
    part = parts[0].shape[1] // lines
    row = jnp.where(first_core, normed[:, :half], normed[:, half:])
    for line in range(lines):
        block = meta
        at = line * part
        for n, values in enumerate(parts):
            tile = values[:, at // 128 * 128 : at // 128 * 128 + 128]
            to = DENSE + n * part
            moved = pltpu.roll(tile, (to - at % 128) % 128, 1)
            inside = jnp.logical_and(meta_lane >= to, meta_lane < to + part)
            block = jnp.where(inside, moved, block)
        send_ref[line, :, :half] = row
        send_ref[line, :, half:] = block.astype(BF16)


def slots_kernel(line_ref, got_ref, send_ref, combine_ref):
    lines, seq_count, width = got_ref.shape
    places, _, half = send_ref.shape
    token_total = lines * seq_count
    capacity = seq_count
    slot_total = places * capacity
    got = got_ref[...].reshape(token_total, width)
    meta = got[:, half:].astype(F32).T
    slot = lax.broadcasted_iota(jnp.int32, (slot_total, token_total), 0)
    token = lax.broadcasted_iota(jnp.int32, (slot_total, token_total), 1)
    expert = (line_ref[0] * places + slot // capacity).astype(F32)
    hit = jnp.zeros((slot_total, token_total), F32)
    gate = jnp.zeros((slot_total, token_total), F32)
    for k in range(6):
        same = meta[k : k + 1] == expert
        hit = jnp.where(same, 1.0, hit)
        gate = jnp.where(same, meta[GATE_HI + k : GATE_HI + k + 1] + meta[GATE_LO + k : GATE_LO + k + 1], gate)
    row = lax.broadcasted_iota(jnp.int32, (token_total, token_total), 0)
    column = lax.broadcasted_iota(jnp.int32, (token_total, token_total), 1)
    earlier = jnp.logical_and(row // seq_count == column // seq_count, row < column)
    rank = jnp.dot(hit.astype(BF16), earlier.astype(BF16), preferred_element_type=F32)
    per_source = capacity // lines
    here = jnp.logical_and(
        token // seq_count == slot % capacity // per_source,
        rank == (slot % per_source).astype(F32),
    )
    chosen = jnp.where(here, hit, 0.0)
    rows = jnp.dot(chosen.astype(BF16), got[:, :half], preferred_element_type=F32)
    send_ref[:, :capacity, :] = rows.astype(BF16).reshape(places, capacity, half)
    for line in range(lines):
        block = got_ref[line, :, half:]
        send_ref[:, capacity:, line * 128 : line * 128 + 128] = jnp.broadcast_to(
            block[None], (places, seq_count, 128)
        )
    weights = jnp.where(here, gate * hit, 0.0).T
    high = weights.astype(BF16)
    combine_ref[:, :slot_total] = high
    combine_ref[:, slot_total:] = (weights - high.astype(F32)).astype(BF16)


def dense_weights(slots_ref, side, at):
    places, rows, _ = slots_ref.shape
    capacity = rows // 2
    lane = pl.multiple_of((side * 4 + at) * 128, 128)
    return slots_ref[:, capacity:, pl.ds(lane, 128)].reshape(places * capacity, 128)


def half_products(side, slots_ref, line_ref, gate_ref, up_ref, dense_ref):
    places, rows, half = slots_ref.shape
    mine = pl.ds(pl.multiple_of(side * half, half), half)
    values = slots_ref[:, : rows // 2, :].reshape(places * rows // 2, half)
    gate = jnp.dot(values, gate_ref[mine, :], preferred_element_type=F32)
    up = jnp.dot(values, up_ref[mine, :], preferred_element_type=F32)
    line = line_ref[:, :, :half].reshape(-1, half)
    block = half // 4
    dense = sum(
        jnp.dot(
            line[:, k * block : (k + 1) * block], dense_weights(dense_ref, side, k), preferred_element_type=F32
        )
        for k in range(4)
    )
    return gate, up, dense


def own_kernel(core_ref, slots_ref, line_ref, gate_ref, up_ref, gate_out, up_out, dense_out):
    gate, up, dense = half_products(core_ref[0], slots_ref, line_ref, gate_ref, up_ref, slots_ref)
    gate_out[...] = gate
    up_out[...] = up
    dense_out[...] = dense


def down_products(side, hidden, dense, down_ref, dense_ref, target_ref):
    slot_total, half = hidden.shape[0], target_ref.shape[1]
    mine = pl.ds(pl.multiple_of(side * half, half), half)
    target_ref[:slot_total, :] = jnp.dot(hidden, down_ref[:, mine], preferred_element_type=F32).astype(BF16)
    block = half // 4
    for k in range(4):
        target_ref[slot_total:, k * block : (k + 1) * block] = lax.dot_general(
            dense, dense_weights(dense_ref, side, k), (((1,), (1,)), ((), ())), preferred_element_type=F32
        ).astype(BF16)


def other_kernel(
    core_ref,
    gate_sum,
    up_sum,
    dense_sum,
    own_ref,
    other_ref,
    line_ref,
    gate_ref,
    up_ref,
    down_ref,
    send_ref,
    hidden_ref,
    dense_ref,
):
    side = 1 - core_ref[0]
    gate, up, dense = half_products(side, other_ref, line_ref, gate_ref, up_ref, own_ref)
    hidden = (jax.nn.silu(gate_sum[...] + gate) * (up_sum[...] + up)).astype(BF16)
    dense += dense_sum[...]
    lane = lax.broadcasted_iota(jnp.int32, dense.shape, 1)
    dense = jnp.where(lane >= 96, jax.nn.silu(pltpu.roll(dense, 64, 1)) * pltpu.roll(dense, 32, 1), 0.0).astype(BF16)
    hidden_ref[...] = hidden
    dense_ref[...] = dense
    down_products(side, hidden, dense, down_ref, own_ref, send_ref)


def keep_kernel(core_ref, hidden_ref, dense_ref, own_ref, down_ref, keep_ref):
    down_products(core_ref[0], hidden_ref[...], dense_ref[...], down_ref, own_ref, keep_ref)


def combine_kernel(back_ref, combine_ref, line_ref, keep_ref, got_ref, send_ref):
    lines, seq_count, half = send_ref.shape
    token_total = lines * seq_count
    slot_total = back_ref.shape[0] * back_ref.shape[1]
    back = back_ref[...].reshape(slot_total, half)
    routed = jnp.dot(combine_ref[:, :slot_total], back, preferred_element_type=F32)
    routed += jnp.dot(combine_ref[:, slot_total:], back, preferred_element_type=F32)
    meta = line_ref[...].reshape(token_total, line_ref.shape[2])[:, half:].astype(F32)
    mix = meta[:, MIX_HI : MIX_HI + 1] + meta[:, MIX_LO : MIX_LO + 1]
    dense = keep_ref[slot_total:, :].astype(F32) + got_ref[slot_total:, :].astype(F32)
    send_ref[...] = (routed + mix * dense).astype(BF16).reshape(lines, seq_count, half)


def shards(
    tokens,
    lengths,
    attn_gain,
    w_query,
    w_key,
    w_value,
    head_bias,
    key_cache,
    value_cache,
    w_attn_out,
    ffn_gain,
    w_router,
    routes,
    w_dense_gate,
    w_dense_up,
    w_dense_down,
    dense_mix,
    w_expert_gate,
    w_expert_up,
    w_expert_down,
):
    seq_count, width = tokens.shape
    half = width // 2
    lines = lax.axis_size(LINE)
    places = lax.axis_size(PLANE)
    slot_total = places * seq_count
    token_total = lines * seq_count
    core = lax.axis_index("tp").astype(jnp.int32).reshape(1)
    line = lax.axis_index(LINE).astype(jnp.int32).reshape(1)
    cache_rows = seq_count * key_cache.shape[2]
    cache_len = key_cache.shape[3]
    attn_own = call(
        attend_kernel,
        jax.ShapeDtypeStruct((seq_count, width), BF16),
        0,
        (
            head_bias.reshape(1, -1),
            lengths.reshape(1, seq_count),
            tokens,
            attn_gain.reshape(1, width),
            w_query,
            key_cache.reshape(cache_rows, cache_len),
            value_cache.reshape(cache_rows, cache_len),
            w_attn_out,
        ),
        52,
        hbm_count=8,
        scratch=(
            pltpu.VMEM((1, head_bias.shape[0]), F32),
            pltpu.VMEM((1, seq_count), jnp.int32),
            pltpu.VMEM(tokens.shape, BF16),
            pltpu.VMEM((1, width), F32),
            pltpu.VMEM(w_query.shape, BF16),
            pltpu.VMEM((cache_rows, cache_len), BF16),
            pltpu.VMEM((cache_rows, cache_len), BF16),
            pltpu.VMEM(w_attn_out.shape, BF16),
            pltpu.SemaphoreType.DMA((11,)),
        ),
    )
    attn_other = lax.ppermute(attn_own, "tp", SWAP)
    line_send, residual = call(
        rows_kernel,
        (
            jax.ShapeDtypeStruct((lines, seq_count, half + 128), BF16),
            jax.ShapeDtypeStruct((seq_count, half), BF16),
        ),
        1,
        (
            core,
            tokens,
            attn_own,
            attn_other,
            ffn_gain.reshape(1, width),
            w_router,
            routes,
            w_dense_gate,
            w_dense_up,
            w_dense_down.T,
            dense_mix.reshape(1, width),
        ),
        8,
    )
    line_own = lax.all_to_all(line_send, LINE, 0, 0, tiled=True)
    line_other = lax.ppermute(line_own, "tp", SWAP)
    slot_send, combine = call(
        slots_kernel,
        (
            jax.ShapeDtypeStruct((places, 2 * seq_count, half), BF16),
            jax.ShapeDtypeStruct((token_total, 2 * slot_total), BF16),
        ),
        1,
        (line, line_own),
        8,
    )
    slot_own = lax.all_to_all(slot_send, PLANE, 0, 0, tiled=True)
    slot_other = lax.ppermute(slot_own, "tp", SWAP)
    weights = (w_expert_gate[0], w_expert_up[0])
    hidden_shape = (slot_total, w_expert_gate.shape[2])
    sums = call(
        own_kernel,
        (jax.ShapeDtypeStruct(hidden_shape, F32),) * 2 + (jax.ShapeDtypeStruct((token_total, 128), F32),),
        1,
        (core, slot_own, line_own, *weights),
        8,
    )
    both_shape = jax.ShapeDtypeStruct((slot_total + token_total, half), BF16)
    send, hidden, dense = call(
        other_kernel,
        (both_shape, jax.ShapeDtypeStruct(hidden_shape, BF16), jax.ShapeDtypeStruct((token_total, 128), BF16)),
        1,
        (core, *sums, slot_own, slot_other, line_other, *weights, w_expert_down[0]),
        12,
    )
    got = lax.ppermute(send, "tp", SWAP)
    keep = call(keep_kernel, both_shape, 1, (core, hidden, dense, slot_own, w_expert_down[0]), 8)
    results = (keep[:slot_total].astype(F32) + got[:slot_total].astype(F32)).astype(BF16)
    back = lax.all_to_all(results.reshape(places, seq_count, half), PLANE, 0, 0, tiled=True)
    partial = call(
        combine_kernel,
        jax.ShapeDtypeStruct((lines, seq_count, half), BF16),
        0,
        (back, combine, line_own, keep, got),
        8,
    )
    parts = lax.all_to_all(partial, LINE, 0, 0, tiled=True)
    layer_out = (residual.astype(F32) + jnp.sum(parts.astype(F32), axis=0)).astype(BF16)
    normed = rms_scale(tokens, attn_gain).astype(BF16)
    new_keys = jnp.dot(normed, w_key, preferred_element_type=F32).astype(BF16)
    new_values = jnp.dot(normed, w_value, preferred_element_type=F32).astype(BF16)
    return (layer_out, new_keys, new_values)


def solution(mesh):
    finer = Mesh(mesh.devices.reshape(8, 4, 4, mesh.shape["tp"]), ("ep_0", "ep_1", "ep_2", "tp"))
    placed = (
        P(EP, None),
        P(EP),
        P(),
        P(None, "tp"),
        P(None, "tp"),
        P(None, "tp"),
        P("tp"),
        P(EP, "tp", None, None),
        P(EP, "tp", None, None),
        P("tp", None),
        P(),
        P(),
        P(EP, None),
        P(EP, "tp"),
        P(EP, "tp"),
        P("tp", EP),
        P(),
        P(EP, None, "tp"),
        P(EP, None, "tp"),
        P(EP, "tp", None),
    )
    return jax.shard_map(
        shards,
        mesh=finer,
        in_specs=placed,
        out_specs=(P(EP, "tp"), P(EP, "tp"), P(EP, "tp")),
        check_vma=False,
    )
```

```python
import jax
import jax.numpy as jnp
from jax import lax
from jax.experimental import pallas as pl
from jax.experimental.pallas import tpu as pltpu
from jax.sharding import Mesh
from jax.sharding import PartitionSpec as P

EP = ("ep_0", "ep_1", "ep_2")
LINE = "ep_0"
PLANE = ("ep_1", "ep_2")
SWAP = ((0, 1), (1, 0))
F32 = jnp.float32
BF16 = jnp.bfloat16

GATE_HI, GATE_LO, MIX_HI, MIX_LO, DENSE = 8, 16, 24, 25, 32


def rms_scale(values, gain):
    wide = values.astype(F32)
    return wide * lax.rsqrt(jnp.mean(wide * wide, axis=-1, keepdims=True) + 1e-06) * gain


def attend_kernel(
    bias_hbm,
    lengths_hbm,
    tokens_hbm,
    gain_hbm,
    query_hbm,
    key_hbm,
    value_hbm,
    out_hbm,
    partial_ref,
    bias_ref,
    lengths_ref,
    tokens_ref,
    gain_ref,
    query_buf,
    key_buf,
    value_buf,
    out_buf,
    sems,
):
    seq_count, width = tokens_ref.shape
    head_total = query_buf.shape[1]
    row_total, cache_len = key_buf.shape
    head_dim = row_total // seq_count
    heads = head_total // head_dim
    copies = []

    def fetch(source, target, pieces):
        size = source.shape[0] // pieces
        made = []
        for n in range(pieces):
            at = pl.ds(n * size, size)
            made.append(pltpu.make_async_copy(source.at[at, :], target.at[at, :], sems.at[len(copies)]))
            copies.append(made[-1])
        return made

    small_copies = [
        fetch(source, target, 1)[0]
        for source, target in (
            (tokens_hbm, tokens_ref),
            (gain_hbm, gain_ref),
            (bias_hbm, bias_ref),
            (lengths_hbm, lengths_ref),
        )
    ]
    query_copies = fetch(query_hbm, query_buf, 2)
    key_copies = fetch(key_hbm, key_buf, 2)
    value_copies = fetch(value_hbm, value_buf, 2)
    out_copies = fetch(out_hbm, out_buf, 1)
    for copy in copies:
        copy.start()

    for copy in small_copies:
        copy.wait()
    normed = rms_scale(tokens_ref[...], gain_ref[...]).astype(BF16)
    row = lax.broadcasted_iota(jnp.int32, (heads * seq_count, 1), 0)
    bias = jnp.zeros((heads * seq_count, 1), F32)
    for h in range(heads):
        bias = jnp.where(row // seq_count == h, bias_ref[:, h : h + 1], bias)
    lengths = jnp.zeros((seq_count, 1), jnp.int32)
    for n in range(seq_count):
        lengths = jnp.where(row[:seq_count] == n, lengths_ref[:, n : n + 1], lengths)
    lengths = jnp.concatenate([lengths] * heads, axis=0)
    lane = lax.broadcasted_iota(jnp.int32, (seq_count, 128), 1)
    low = lane < head_dim
    own = (
        lax.broadcasted_iota(jnp.int32, (seq_count, row_total), 1) // head_dim
        == lax.broadcasted_iota(jnp.int32, (seq_count, row_total), 0)
    )
    span = 256
    after_mask = (
        lax.broadcasted_iota(jnp.int32, (span, span), 0) > lax.broadcasted_iota(jnp.int32, (span, span), 1)
    ).astype(BF16)

    queries = jnp.zeros((seq_count, head_total), F32)
    piece = width // len(query_copies)
    for n, copy in enumerate(query_copies):
        copy.wait()
        at = slice(n * piece, (n + 1) * piece)
        queries += jnp.dot(normed[:, at], query_buf[at, :], preferred_element_type=F32)
    queries = queries.astype(BF16).astype(F32)
    spread = []
    for h in range(heads):
        tile = queries[:, h // 2 * 128 : h // 2 * 128 + 128]
        turned = pltpu.roll(tile, head_dim, 1)
        both = jnp.where(low, tile, turned) if h % 2 == 0 else jnp.where(low, turned, tile)
        wide = jnp.concatenate([both] * (row_total // 128), axis=1)
        spread.append(jnp.where(own, wide, 0.0).astype(BF16))
    spread = jnp.concatenate(spread, axis=0)

    scores = None
    piece = row_total // len(key_copies)
    for n, copy in enumerate(key_copies):
        copy.wait()
        at = slice(n * piece, (n + 1) * piece)
        part = jnp.dot(spread[:, at], key_buf[at, :], preferred_element_type=F32)
        scores = part if scores is None else scores + part
    later = jnp.zeros((heads * seq_count, 1), F32)
    sticks = []
    for block in reversed(range(cache_len // span)):
        score = scores[:, block * span : (block + 1) * span] * head_dim ** (-0.5) + bias
        position = lax.broadcasted_iota(jnp.int32, score.shape, 1) + block * span
        visible = position < lengths
        soft = jnp.log1p(jnp.exp(-jnp.abs(score)))
        log_keep = jnp.where(visible, -(jnp.maximum(score, 0.0) + soft), 0.0)
        high = log_keep.astype(BF16)
        rest = (log_keep - high.astype(F32)).astype(BF16)
        log_after = jnp.dot(high, after_mask, preferred_element_type=F32)
        log_after += jnp.dot(rest, after_mask, preferred_element_type=F32)
        weight = jnp.exp(jnp.minimum(score, 0.0) - soft + (log_after + later))
        sticks.append(jnp.where(visible, weight, 0.0).astype(BF16))
        later += jnp.sum(log_keep, axis=-1, keepdims=True)
    sticks = jnp.concatenate(sticks[::-1], axis=1)

    read = []
    piece = row_total // len(value_copies)
    for n, copy in enumerate(value_copies):
        copy.wait()
        read.append(
            lax.dot_general(
                sticks,
                value_buf[n * piece : (n + 1) * piece, :],
                (((1,), (1,)), ((), ())),
                preferred_element_type=F32,
            )
        )
    read = jnp.concatenate(read, axis=1)
    folded = []
    for h in range(heads):
        mine = jnp.where(own, read[h * seq_count : (h + 1) * seq_count], 0.0)
        tile = mine[:, :128]
        for n in range(1, row_total // 128):
            tile += mine[:, n * 128 : (n + 1) * 128]
        folded.append(tile + pltpu.roll(tile, head_dim, 1))
    heads_out = jnp.concatenate(
        [jnp.where(low, folded[h], folded[h + 1]) for h in range(0, heads, 2)], axis=1
    ).astype(BF16)
    for copy in out_copies:
        copy.wait()
    partial_ref[...] = jnp.dot(heads_out, out_buf[...], preferred_element_type=F32).astype(BF16)


def call(kernel, out_shape, smem_count, inputs, limit, hbm_count=0, scratch=()):
    in_specs = [pl.BlockSpec(memory_space=pltpu.SMEM)] * smem_count
    in_specs += [pl.BlockSpec(memory_space=pltpu.VMEM)] * (len(inputs) - smem_count - hbm_count)
    in_specs += [pl.BlockSpec(memory_space=pltpu.HBM)] * hbm_count
    held = [pltpu.with_memory_space_constraint(x, pltpu.HBM) for x in inputs[len(inputs) - hbm_count :]]
    return pl.pallas_call(
        kernel,
        out_shape=out_shape,
        in_specs=in_specs,
        out_specs=jax.tree.map(lambda _: pl.BlockSpec(memory_space=pltpu.VMEM), out_shape),
        scratch_shapes=scratch,
        compiler_params=pltpu.CompilerParams(vmem_limit_bytes=limit * 1024 * 1024),
    )(*inputs[: len(inputs) - hbm_count], *held)


def rows_kernel(
    core_ref,
    line_ref,
    tokens_ref,
    own_ref,
    other_ref,
    gain_ref,
    router_ref,
    routes_ref,
    gate_ref,
    up_ref,
    down_ref,
    mix_ref,
    send_ref,
    residual_ref,
):
    first_core = core_ref[0] == 0
    lines, seq_count, _ = send_ref.shape
    half = residual_ref.shape[1]
    attn = own_ref[...].astype(F32) + other_ref[...].astype(F32)
    residual = (tokens_ref[...].astype(F32) + attn).astype(BF16)
    normed = rms_scale(residual, gain_ref[...]).astype(BF16)
    residual_ref[...] = jnp.where(first_core, residual[:, :half], residual[:, half:])
    probs = jax.nn.sigmoid(jnp.dot(normed, router_ref[...], preferred_element_type=F32))
    mix = jax.nn.sigmoid(jnp.sum(normed.astype(F32) * mix_ref[...], axis=-1, keepdims=True))
    routes = routes_ref[...]
    lane = lax.broadcasted_iota(jnp.int32, probs.shape, 1)
    picked = [
        jnp.sum(jnp.where(lane == routes[:, k : k + 1], probs, 0.0), axis=-1, keepdims=True)
        for k in range(routes.shape[1])
    ]
    total = sum(picked[1:], picked[0])
    meta_lane = lax.broadcasted_iota(jnp.int32, (seq_count, 128), 1)
    meta = jnp.zeros((seq_count, 128), F32)

    def put(meta, at, value):
        return jnp.where(meta_lane == at, value, meta)

    for k, one in enumerate(picked):
        gate = one / total * 2.5
        high = gate.astype(BF16).astype(F32)
        meta = put(meta, k, routes[:, k : k + 1].astype(F32))
        meta = put(meta, GATE_HI + k, high)
        meta = put(meta, GATE_LO + k, gate - high)
    mix_high = mix.astype(BF16).astype(F32)
    meta = put(put(meta, MIX_HI, mix_high), MIX_LO, mix - mix_high)
    parts = [ref[...].astype(F32) for ref in (gate_ref, up_ref, down_ref)]
    part = parts[0].shape[1] // lines
    row = jnp.where(first_core, normed[:, :half], normed[:, half:])
    for line in range(lines):
        block = meta
        at = line * part
        for n, values in enumerate(parts):
            tile = values[:, at // 128 * 128 : at // 128 * 128 + 128]
            to = DENSE + n * part
            moved = pltpu.roll(tile, (to - at % 128) % 128, 1)
            inside = jnp.logical_and(meta_lane >= to, meta_lane < to + part)
            block = jnp.where(inside, moved, block)
        send_ref[line, :, :half] = row
        send_ref[line, :, half:] = block.astype(BF16)


def slots_kernel(line_ref, got_ref, send_ref, combine_ref):
    lines, seq_count, width = got_ref.shape
    places = send_ref.shape[0]
    half = width - 128
    token_total = lines * seq_count
    capacity = seq_count
    slot_total = places * capacity
    got = got_ref[...].reshape(token_total, width)
    meta = got[:, half:].astype(F32).T
    slot = lax.broadcasted_iota(jnp.int32, (slot_total, token_total), 0)
    token = lax.broadcasted_iota(jnp.int32, (slot_total, token_total), 1)
    expert = (line_ref[0] * places + slot // capacity).astype(F32)
    hit = jnp.zeros((slot_total, token_total), F32)
    gate = jnp.zeros((slot_total, token_total), F32)
    for k in range(6):
        same = meta[k : k + 1] == expert
        hit = jnp.where(same, 1.0, hit)
        gate = jnp.where(same, meta[GATE_HI + k : GATE_HI + k + 1] + meta[GATE_LO + k : GATE_LO + k + 1], gate)
    row = lax.broadcasted_iota(jnp.int32, (token_total, token_total), 0)
    column = lax.broadcasted_iota(jnp.int32, (token_total, token_total), 1)
    earlier = jnp.logical_and(row // seq_count == column // seq_count, row < column)
    rank = jnp.dot(hit.astype(BF16), earlier.astype(BF16), preferred_element_type=F32)
    per_source = capacity // lines
    here = jnp.logical_and(
        token // seq_count == slot % capacity // per_source,
        rank == (slot % per_source).astype(F32),
    )
    chosen = jnp.where(here, hit, 0.0)
    rows = jnp.dot(chosen.astype(BF16), got[:, :half], preferred_element_type=F32)
    send_ref[:, :, :half] = rows.astype(BF16).reshape(places, capacity, half)
    group = (lax.broadcasted_iota(jnp.int32, (seq_count, 128), 1)) // 32
    for n in range(3):
        for first in range(0, lines, 4):
            tile = jnp.zeros((seq_count, 128), F32)
            for k in range(4):
                block = got[(first + k) * seq_count : (first + k + 1) * seq_count, half:].astype(F32)
                moved = pltpu.roll(block, (k * 32 - DENSE - n * 32) % 128, 1)
                tile = jnp.where(group == k, moved, tile)
            at = half + (n * lines + first) * 32
            send_ref[:, :, at : at + 128] = jnp.broadcast_to(tile.astype(BF16)[None], (places, seq_count, 128))
    weights = jnp.where(here, gate * hit, 0.0).T
    high = weights.astype(BF16)
    combine_ref[:, :slot_total] = high
    combine_ref[:, slot_total:] = (weights - high.astype(F32)).astype(BF16)


def dense_weights(slots_ref, half, part, line):
    lanes = 32 * 8
    at = pl.multiple_of(half + part * lanes + line // 4 * 128, 128)
    return slots_ref[:, :, pl.ds(at, 128)].reshape(-1, 128)


def lane_group(shape):
    return lax.broadcasted_iota(jnp.int32, shape, 1) // 32


def half_products(side, slots_ref, line_ref, gate_ref, up_ref, dense_ref):
    half = line_ref.shape[2] - 128
    mine = pl.ds(pl.multiple_of(side * half, half), half)
    values = slots_ref[:, :, :half].reshape(-1, half)
    gate = jnp.dot(values, gate_ref[mine, :], preferred_element_type=F32)
    up = jnp.dot(values, up_ref[mine, :], preferred_element_type=F32)
    rows = line_ref[:, :, :half].reshape(-1, half)
    block = half // 4
    group = lane_group((rows.shape[0], 128))
    dense = []
    for part in range(2):
        weights = dense_weights(dense_ref, half, part, side * 4)
        total = jnp.zeros(group.shape, F32)
        for k in range(4):
            product = jnp.dot(rows[:, k * block : (k + 1) * block], weights, preferred_element_type=F32)
            total += jnp.where(group == k, product, 0.0)
        dense.append(total)
    return gate, up, dense


def own_kernel(core_ref, slots_ref, line_ref, gate_ref, up_ref, gate_out, up_out, dense_out):
    gate, up, dense = half_products(core_ref[0], slots_ref, line_ref, gate_ref, up_ref, slots_ref)
    gate_out[...] = gate
    up_out[...] = up
    for n, values in enumerate(dense):
        dense_out[n] = values


def down_products(side, hidden, dense, down_ref, dense_ref, target_ref):
    slot_total, half = hidden.shape[0], target_ref.shape[1]
    mine = pl.ds(pl.multiple_of(side * half, half), half)
    target_ref[:slot_total, :] = jnp.dot(hidden, down_ref[:, mine], preferred_element_type=F32).astype(BF16)
    block = half // 4
    weights = dense_weights(dense_ref, half, 2, side * 4)
    group = lane_group(dense.shape)
    for k in range(4):
        target_ref[slot_total:, k * block : (k + 1) * block] = lax.dot_general(
            jnp.where(group == k, dense, 0.0).astype(BF16),
            weights,
            (((1,), (1,)), ((), ())),
            preferred_element_type=F32,
        ).astype(BF16)


def other_kernel(
    core_ref,
    gate_sum,
    up_sum,
    dense_sum,
    own_ref,
    other_ref,
    line_ref,
    gate_ref,
    up_ref,
    down_ref,
    send_ref,
    hidden_ref,
    dense_ref,
):
    side = 1 - core_ref[0]
    gate, up, dense = half_products(side, other_ref, line_ref, gate_ref, up_ref, own_ref)
    hidden = (jax.nn.silu(gate_sum[...] + gate) * (up_sum[...] + up)).astype(BF16)
    sums = []
    for n, values in enumerate(dense):
        total = values + dense_sum[n]
        total += pltpu.roll(total, 64, 1)
        sums.append(total + pltpu.roll(total, 32, 1))
    dense = (jax.nn.silu(sums[0]) * sums[1]).astype(BF16)
    hidden_ref[...] = hidden
    dense_ref[...] = dense
    down_products(side, hidden, dense.astype(F32), down_ref, own_ref, send_ref)


def keep_kernel(
    core_ref,
    hidden_ref,
    dense_ref,
    own_ref,
    down_ref,
    tokens_ref,
    gain_ref,
    key_ref,
    value_ref,
    keep_ref,
    keys_ref,
    values_ref,
):
    down_products(core_ref[0], hidden_ref[...], dense_ref[...].astype(F32), down_ref, own_ref, keep_ref)
    normed = rms_scale(tokens_ref[...], gain_ref[...]).astype(BF16)
    for weight_ref, target_ref in ((key_ref, keys_ref), (value_ref, values_ref)):
        target_ref[...] = lax.dot_general(
            normed, weight_ref[...], (((1,), (1,)), ((), ())), preferred_element_type=F32
        ).astype(BF16)


def combine_kernel(back_ref, combine_ref, line_ref, keep_ref, got_ref, send_ref):
    lines, seq_count, half = send_ref.shape
    token_total = lines * seq_count
    slot_total = back_ref.shape[0] * back_ref.shape[1]
    back = back_ref[...].reshape(slot_total, half)
    routed = jnp.dot(combine_ref[:, :slot_total], back, preferred_element_type=F32)
    routed += jnp.dot(combine_ref[:, slot_total:], back, preferred_element_type=F32)
    meta = line_ref[...].reshape(token_total, line_ref.shape[2])[:, half:].astype(F32)
    mix = meta[:, MIX_HI : MIX_HI + 1] + meta[:, MIX_LO : MIX_LO + 1]
    dense = keep_ref[slot_total:, :].astype(F32) + got_ref[slot_total:, :].astype(F32)
    send_ref[...] = (routed + mix * dense).astype(BF16).reshape(lines, seq_count, half)


def shards(
    tokens,
    lengths,
    attn_gain,
    w_query,
    w_key,
    w_value,
    head_bias,
    key_cache,
    value_cache,
    w_attn_out,
    ffn_gain,
    w_router,
    routes,
    w_dense_gate,
    w_dense_up,
    w_dense_down,
    dense_mix,
    w_expert_gate,
    w_expert_up,
    w_expert_down,
):
    seq_count, width = tokens.shape
    half = width // 2
    lines = lax.axis_size(LINE)
    places = lax.axis_size(PLANE)
    slot_total = places * seq_count
    token_total = lines * seq_count
    core = lax.axis_index("tp").astype(jnp.int32).reshape(1)
    line = lax.axis_index(LINE).astype(jnp.int32).reshape(1)
    cache_rows = seq_count * key_cache.shape[2]
    cache_len = key_cache.shape[3]
    attn_own = call(
        attend_kernel,
        jax.ShapeDtypeStruct((seq_count, width), BF16),
        0,
        (
            head_bias.reshape(1, -1),
            lengths.reshape(1, seq_count),
            tokens,
            attn_gain.reshape(1, width),
            w_query,
            key_cache.reshape(cache_rows, cache_len),
            value_cache.reshape(cache_rows, cache_len),
            w_attn_out,
        ),
        24,
        hbm_count=8,
        scratch=(
            pltpu.VMEM((1, head_bias.shape[0]), F32),
            pltpu.VMEM((1, seq_count), jnp.int32),
            pltpu.VMEM(tokens.shape, BF16),
            pltpu.VMEM((1, width), F32),
            pltpu.VMEM(w_query.shape, BF16),
            pltpu.VMEM((cache_rows, cache_len), BF16),
            pltpu.VMEM((cache_rows, cache_len), BF16),
            pltpu.VMEM(w_attn_out.shape, BF16),
            pltpu.SemaphoreType.DMA((11,)),
        ),
    )
    attn_other = lax.ppermute(attn_own, "tp", SWAP)
    line_send, residual = call(
        rows_kernel,
        (
            jax.ShapeDtypeStruct((lines, seq_count, half + 128), BF16),
            jax.ShapeDtypeStruct((seq_count, half), BF16),
        ),
        2,
        (
            core,
            line,
            tokens,
            attn_own,
            attn_other,
            ffn_gain.reshape(1, width),
            w_router,
            routes,
            w_dense_gate,
            w_dense_up,
            w_dense_down.T,
            dense_mix.reshape(1, width),
        ),
        8,
    )
    line_own = lax.all_to_all(line_send, LINE, 0, 0, tiled=True)
    line_other = lax.ppermute(line_own, "tp", SWAP)
    slot_send, combine = call(
        slots_kernel,
        (
            jax.ShapeDtypeStruct((places, seq_count, half + 96 * lines), BF16),
            jax.ShapeDtypeStruct((token_total, 2 * slot_total), BF16),
        ),
        1,
        (line, line_own),
        8,
    )
    slot_own = lax.all_to_all(slot_send, PLANE, 0, 0, tiled=True)
    slot_other = lax.ppermute(slot_own, "tp", SWAP)
    weights = (w_expert_gate[0], w_expert_up[0])
    hidden_shape = (slot_total, w_expert_gate.shape[2])
    sums = call(
        own_kernel,
        (jax.ShapeDtypeStruct(hidden_shape, F32),) * 2 + (jax.ShapeDtypeStruct((2, token_total, 128), F32),),
        1,
        (core, slot_own, line_own, *weights),
        8,
    )
    both_shape = jax.ShapeDtypeStruct((slot_total + token_total, half), BF16)
    send, hidden, dense = call(
        other_kernel,
        (both_shape, jax.ShapeDtypeStruct(hidden_shape, BF16), jax.ShapeDtypeStruct((token_total, 128), BF16)),
        1,
        (core, *sums, slot_own, slot_other, line_other, *weights, w_expert_down[0]),
        12,
    )
    got = lax.ppermute(send, "tp", SWAP)
    new_shape = jax.ShapeDtypeStruct((seq_count, w_key.shape[1]), BF16)
    keep, new_keys, new_values = call(
        keep_kernel,
        (both_shape, new_shape, new_shape),
        1,
        (
            core,
            hidden,
            dense,
            slot_own,
            w_expert_down[0],
            tokens,
            attn_gain.reshape(1, width),
            w_key.T,
            w_value.T,
        ),
        8,
    )
    results = (keep[:slot_total].astype(F32) + got[:slot_total].astype(F32)).astype(BF16)
    back = lax.all_to_all(results.reshape(places, seq_count, half), PLANE, 0, 0, tiled=True)
    partial = call(
        combine_kernel,
        jax.ShapeDtypeStruct((lines, seq_count, half), BF16),
        0,
        (back, combine, line_own, keep, got),
        8,
    )
    parts = lax.all_to_all(partial, LINE, 0, 0, tiled=True)
    layer_out = (residual.astype(F32) + jnp.sum(parts.astype(F32), axis=0)).astype(BF16)
    return (layer_out, new_keys, new_values)


def solution(mesh):
    finer = Mesh(mesh.devices.reshape(8, 4, 4, mesh.shape["tp"]), ("ep_0", "ep_1", "ep_2", "tp"))
    placed = (
        P(EP, None),
        P(EP),
        P(),
        P(None, "tp"),
        P(None, "tp"),
        P(None, "tp"),
        P("tp"),
        P(EP, "tp", None, None),
        P(EP, "tp", None, None),
        P("tp", None),
        P(),
        P(),
        P(EP, None),
        P(EP, "tp"),
        P(EP, "tp"),
        P("tp", EP),
        P(),
        P(EP, None, "tp"),
        P(EP, None, "tp"),
        P(EP, "tp", None),
    )
    return jax.shard_map(
        shards,
        mesh=finer,
        in_specs=placed,
        out_specs=(P(EP, "tp"), P(EP, "tp"), P(EP, "tp")),
        check_vma=False,
    )
```

```python
import jax
import jax.numpy as jnp
from jax import lax
from jax.experimental import pallas as pl
from jax.experimental.pallas import tpu as pltpu
from jax.sharding import Mesh
from jax.sharding import PartitionSpec as P

EP = ("ep_0", "ep_1", "ep_2")
LINE = "ep_0"
PLANE = ("ep_1", "ep_2")
SWAP = ((0, 1), (1, 0))
F32 = jnp.float32
BF16 = jnp.bfloat16

GATE_HI, GATE_LO, MIX_HI, MIX_LO, DENSE = 8, 16, 24, 25, 32


def rms_scale(values, gain):
    wide = values.astype(F32)
    return wide * lax.rsqrt(jnp.mean(wide * wide, axis=-1, keepdims=True) + 1e-06) * gain


def attend_kernel(
    bias_hbm,
    lengths_hbm,
    tokens_hbm,
    gain_hbm,
    query_hbm,
    key_hbm,
    value_hbm,
    out_hbm,
    partial_ref,
    bias_ref,
    lengths_ref,
    tokens_ref,
    gain_ref,
    query_buf,
    key_buf,
    value_buf,
    out_buf,
    sems,
):
    seq_count, width = tokens_ref.shape
    head_total = query_buf.shape[1]
    row_total, cache_len = key_buf.shape
    head_dim = row_total // seq_count
    heads = head_total // head_dim
    copies = []

    def fetch(source, target, pieces):
        size = source.shape[0] // pieces
        made = []
        for n in range(pieces):
            at = pl.ds(n * size, size)
            made.append(pltpu.make_async_copy(source.at[at, :], target.at[at, :], sems.at[len(copies)]))
            copies.append(made[-1])
        return made

    small_copies = [
        fetch(source, target, 1)[0]
        for source, target in (
            (tokens_hbm, tokens_ref),
            (gain_hbm, gain_ref),
            (bias_hbm, bias_ref),
            (lengths_hbm, lengths_ref),
        )
    ]
    query_copies = fetch(query_hbm, query_buf, 2)
    key_copies = fetch(key_hbm, key_buf, 2)
    value_copies = fetch(value_hbm, value_buf, 2)
    out_copies = fetch(out_hbm, out_buf, 1)
    for copy in copies:
        copy.start()

    for copy in small_copies:
        copy.wait()
    normed = rms_scale(tokens_ref[...], gain_ref[...]).astype(BF16)
    row = lax.broadcasted_iota(jnp.int32, (heads * seq_count, 1), 0)
    bias = jnp.zeros((heads * seq_count, 1), F32)
    for h in range(heads):
        bias = jnp.where(row // seq_count == h, bias_ref[:, h : h + 1], bias)
    lengths = jnp.zeros((seq_count, 1), jnp.int32)
    for n in range(seq_count):
        lengths = jnp.where(row[:seq_count] == n, lengths_ref[:, n : n + 1], lengths)
    lengths = jnp.concatenate([lengths] * heads, axis=0)
    lane = lax.broadcasted_iota(jnp.int32, (seq_count, 128), 1)
    low = lane < head_dim
    own = (
        lax.broadcasted_iota(jnp.int32, (seq_count, row_total), 1) // head_dim
        == lax.broadcasted_iota(jnp.int32, (seq_count, row_total), 0)
    )
    span = 256
    after_mask = (
        lax.broadcasted_iota(jnp.int32, (span, span), 0) > lax.broadcasted_iota(jnp.int32, (span, span), 1)
    ).astype(BF16)

    queries = jnp.zeros((seq_count, head_total), F32)
    piece = width // len(query_copies)
    for n, copy in enumerate(query_copies):
        copy.wait()
        at = slice(n * piece, (n + 1) * piece)
        queries += jnp.dot(normed[:, at], query_buf[at, :], preferred_element_type=F32)
    queries = queries.astype(BF16).astype(F32)
    spread = []
    for h in range(heads):
        tile = queries[:, h // 2 * 128 : h // 2 * 128 + 128]
        turned = pltpu.roll(tile, head_dim, 1)
        both = jnp.where(low, tile, turned) if h % 2 == 0 else jnp.where(low, turned, tile)
        wide = jnp.concatenate([both] * (row_total // 128), axis=1)
        spread.append(jnp.where(own, wide, 0.0).astype(BF16))
    spread = jnp.concatenate(spread, axis=0)

    scores = None
    piece = row_total // len(key_copies)
    for n, copy in enumerate(key_copies):
        copy.wait()
        at = slice(n * piece, (n + 1) * piece)
        part = jnp.dot(spread[:, at], key_buf[at, :], preferred_element_type=F32)
        scores = part if scores is None else scores + part
    later = jnp.zeros((heads * seq_count, 1), F32)
    sticks = []
    for block in reversed(range(cache_len // span)):
        score = scores[:, block * span : (block + 1) * span] * head_dim ** (-0.5) + bias
        position = lax.broadcasted_iota(jnp.int32, score.shape, 1) + block * span
        visible = position < lengths
        soft = jnp.log1p(jnp.exp(-jnp.abs(score)))
        log_keep = jnp.where(visible, -(jnp.maximum(score, 0.0) + soft), 0.0)
        high = log_keep.astype(BF16)
        rest = (log_keep - high.astype(F32)).astype(BF16)
        log_after = jnp.dot(high, after_mask, preferred_element_type=F32)
        log_after += jnp.dot(rest, after_mask, preferred_element_type=F32)
        weight = jnp.exp(jnp.minimum(score, 0.0) - soft + (log_after + later))
        sticks.append(jnp.where(visible, weight, 0.0).astype(BF16))
        later += jnp.sum(log_keep, axis=-1, keepdims=True)
    sticks = jnp.concatenate(sticks[::-1], axis=1)

    read = []
    piece = row_total // len(value_copies)
    for n, copy in enumerate(value_copies):
        copy.wait()
        read.append(
            lax.dot_general(
                sticks,
                value_buf[n * piece : (n + 1) * piece, :],
                (((1,), (1,)), ((), ())),
                preferred_element_type=F32,
            )
        )
    read = jnp.concatenate(read, axis=1)
    folded = []
    for h in range(heads):
        mine = jnp.where(own, read[h * seq_count : (h + 1) * seq_count], 0.0)
        tile = mine[:, :128]
        for n in range(1, row_total // 128):
            tile += mine[:, n * 128 : (n + 1) * 128]
        folded.append(tile + pltpu.roll(tile, head_dim, 1))
    heads_out = jnp.concatenate(
        [jnp.where(low, folded[h], folded[h + 1]) for h in range(0, heads, 2)], axis=1
    ).astype(BF16)
    for copy in out_copies:
        copy.wait()
    partial_ref[...] = jnp.dot(heads_out, out_buf[...], preferred_element_type=F32).astype(BF16)


def call(kernel, out_shape, smem_count, inputs, limit, hbm_count=0, scratch=()):
    in_specs = [pl.BlockSpec(memory_space=pltpu.SMEM)] * smem_count
    in_specs += [pl.BlockSpec(memory_space=pltpu.VMEM)] * (len(inputs) - smem_count - hbm_count)
    in_specs += [pl.BlockSpec(memory_space=pltpu.HBM)] * hbm_count
    held = [pltpu.with_memory_space_constraint(x, pltpu.HBM) for x in inputs[len(inputs) - hbm_count :]]
    return pl.pallas_call(
        kernel,
        out_shape=out_shape,
        in_specs=in_specs,
        out_specs=jax.tree.map(lambda _: pl.BlockSpec(memory_space=pltpu.VMEM), out_shape),
        scratch_shapes=scratch,
        compiler_params=pltpu.CompilerParams(vmem_limit_bytes=limit * 1024 * 1024),
    )(*inputs[: len(inputs) - hbm_count], *held)


def rows_kernel(
    core_ref,
    line_ref,
    tokens_ref,
    own_ref,
    other_ref,
    gain_ref,
    router_ref,
    routes_ref,
    gate_ref,
    up_ref,
    down_ref,
    mix_ref,
    send_ref,
    residual_ref,
):
    first_core = core_ref[0] == 0
    lines, seq_count, _ = send_ref.shape
    half = residual_ref.shape[1]
    attn = own_ref[...].astype(F32) + other_ref[...].astype(F32)
    residual = (tokens_ref[...].astype(F32) + attn).astype(BF16)
    normed = rms_scale(residual, gain_ref[...]).astype(BF16)
    residual_ref[...] = jnp.where(first_core, residual[:, :half], residual[:, half:])
    probs = jax.nn.sigmoid(jnp.dot(normed, router_ref[...], preferred_element_type=F32))
    mix = jax.nn.sigmoid(jnp.sum(normed.astype(F32) * mix_ref[...], axis=-1, keepdims=True))
    routes = routes_ref[...]
    lane = lax.broadcasted_iota(jnp.int32, probs.shape, 1)
    picked = [
        jnp.sum(jnp.where(lane == routes[:, k : k + 1], probs, 0.0), axis=-1, keepdims=True)
        for k in range(routes.shape[1])
    ]
    total = sum(picked[1:], picked[0])
    meta_lane = lax.broadcasted_iota(jnp.int32, (seq_count, 128), 1)
    meta = jnp.zeros((seq_count, 128), F32)

    def put(meta, at, value):
        return jnp.where(meta_lane == at, value, meta)

    for k, one in enumerate(picked):
        gate = one / total * 2.5
        high = gate.astype(BF16).astype(F32)
        meta = put(meta, k, routes[:, k : k + 1].astype(F32))
        meta = put(meta, GATE_HI + k, high)
        meta = put(meta, GATE_LO + k, gate - high)
    mix_high = mix.astype(BF16).astype(F32)
    meta = put(put(meta, MIX_HI, mix_high), MIX_LO, mix - mix_high)
    parts = [ref[...].astype(F32) for ref in (gate_ref, up_ref, down_ref)]
    part = parts[0].shape[1] // lines
    row = jnp.where(first_core, normed[:, :half], normed[:, half:])
    for line in range(lines):
        block = meta
        at = line * part
        for n, values in enumerate(parts):
            tile = values[:, at // 128 * 128 : at // 128 * 128 + 128]
            to = DENSE + n * part
            moved = pltpu.roll(tile, (to - at % 128) % 128, 1)
            inside = jnp.logical_and(meta_lane >= to, meta_lane < to + part)
            block = jnp.where(inside, moved, block)
        send_ref[line, :, :half] = row
        send_ref[line, :, half:] = block.astype(BF16)


def slots_kernel(line_ref, got_ref, send_ref, combine_ref):
    lines, seq_count, width = got_ref.shape
    places = send_ref.shape[0]
    half = width - 128
    token_total = lines * seq_count
    capacity = seq_count
    slot_total = places * capacity
    got = got_ref[...].reshape(token_total, width)
    meta = got[:, half:].astype(F32).T
    slot = lax.broadcasted_iota(jnp.int32, (slot_total, token_total), 0)
    token = lax.broadcasted_iota(jnp.int32, (slot_total, token_total), 1)
    expert = (line_ref[0] * places + slot // capacity).astype(F32)
    hit = jnp.zeros((slot_total, token_total), F32)
    gate = jnp.zeros((slot_total, token_total), F32)
    for k in range(6):
        same = meta[k : k + 1] == expert
        hit = jnp.where(same, 1.0, hit)
        gate = jnp.where(same, meta[GATE_HI + k : GATE_HI + k + 1] + meta[GATE_LO + k : GATE_LO + k + 1], gate)
    row = lax.broadcasted_iota(jnp.int32, (token_total, token_total), 0)
    column = lax.broadcasted_iota(jnp.int32, (token_total, token_total), 1)
    earlier = jnp.logical_and(row // seq_count == column // seq_count, row < column)
    rank = jnp.dot(hit.astype(BF16), earlier.astype(BF16), preferred_element_type=F32)
    per_source = capacity // lines
    here = jnp.logical_and(
        token // seq_count == slot % capacity // per_source,
        rank == (slot % per_source).astype(F32),
    )
    chosen = jnp.where(here, hit, 0.0)
    rows = jnp.dot(chosen.astype(BF16), got[:, :half], preferred_element_type=F32)
    send_ref[:, :, :half] = rows.astype(BF16).reshape(places, capacity, half)
    group = (lax.broadcasted_iota(jnp.int32, (seq_count, 128), 1)) // 32
    for n in range(3):
        for first in range(0, lines, 4):
            tile = jnp.zeros((seq_count, 128), F32)
            for k in range(4):
                block = got[(first + k) * seq_count : (first + k + 1) * seq_count, half:].astype(F32)
                moved = pltpu.roll(block, (k * 32 - DENSE - n * 32) % 128, 1)
                tile = jnp.where(group == k, moved, tile)
            at = half + (n * lines + first) * 32
            send_ref[:, :, at : at + 128] = jnp.broadcast_to(tile.astype(BF16)[None], (places, seq_count, 128))
    weights = jnp.where(here, gate * hit, 0.0).T
    high = weights.astype(BF16)
    combine_ref[:, :slot_total] = high
    combine_ref[:, slot_total:] = (weights - high.astype(F32)).astype(BF16)


def dense_weights(slots_ref, half, part, line):
    lanes = 32 * 8
    at = pl.multiple_of(half + part * lanes + line // 4 * 128, 128)
    return slots_ref[:, :, pl.ds(at, 128)].reshape(-1, 128)


def lane_group(shape):
    return lax.broadcasted_iota(jnp.int32, shape, 1) // 32


def half_products(side, slots_ref, line_ref, gate_ref, up_ref, dense_ref):
    half = line_ref.shape[2] - 128
    mine = pl.ds(pl.multiple_of(side * half, half), half)
    values = slots_ref[:, :, :half].reshape(-1, half)
    gate = jnp.dot(values, gate_ref[mine, :], preferred_element_type=F32)
    up = jnp.dot(values, up_ref[mine, :], preferred_element_type=F32)
    rows = line_ref[:, :, :half].reshape(-1, half)
    block = half // 4
    group = lane_group((rows.shape[0], 128))
    dense = []
    for part in range(2):
        weights = dense_weights(dense_ref, half, part, side * 4)
        total = jnp.zeros(group.shape, F32)
        for k in range(4):
            product = jnp.dot(rows[:, k * block : (k + 1) * block], weights, preferred_element_type=F32)
            total += jnp.where(group == k, product, 0.0)
        dense.append(total)
    return gate, up, dense


def own_kernel(core_ref, slots_ref, line_ref, gate_ref, up_ref, gate_out, up_out, dense_out):
    gate, up, dense = half_products(core_ref[0], slots_ref, line_ref, gate_ref, up_ref, slots_ref)
    gate_out[...] = gate
    up_out[...] = up
    for n, values in enumerate(dense):
        dense_out[n] = values


def down_products(side, hidden, dense, down_ref, dense_ref, target_ref, line_target):
    half = target_ref.shape[1]
    mine = pl.ds(pl.multiple_of(side * half, half), half)
    target_ref[...] = jnp.dot(hidden, down_ref[:, mine], preferred_element_type=F32).astype(BF16)
    block = half // 4
    weights = dense_weights(dense_ref, half, 2, side * 4)
    group = lane_group(dense.shape)
    for k in range(4):
        line_target[:, k * block : (k + 1) * block] = lax.dot_general(
            jnp.where(group == k, dense, 0.0).astype(BF16),
            weights,
            (((1,), (1,)), ((), ())),
            preferred_element_type=F32,
        ).astype(BF16)


def other_kernel(
    core_ref,
    gate_sum,
    up_sum,
    dense_sum,
    own_ref,
    other_ref,
    line_ref,
    gate_ref,
    up_ref,
    down_ref,
    send_ref,
    line_send_ref,
    hidden_ref,
    dense_ref,
):
    side = 1 - core_ref[0]
    gate, up, dense = half_products(side, other_ref, line_ref, gate_ref, up_ref, own_ref)
    hidden = (jax.nn.silu(gate_sum[...] + gate) * (up_sum[...] + up)).astype(BF16)
    sums = []
    for n, values in enumerate(dense):
        total = values + dense_sum[n]
        total += pltpu.roll(total, 64, 1)
        sums.append(total + pltpu.roll(total, 32, 1))
    dense = (jax.nn.silu(sums[0]) * sums[1]).astype(BF16)
    hidden_ref[...] = hidden
    dense_ref[...] = dense
    down_products(side, hidden, dense.astype(F32), down_ref, own_ref, send_ref, line_send_ref)


def keep_kernel(
    core_ref,
    hidden_ref,
    dense_ref,
    own_ref,
    down_ref,
    tokens_ref,
    gain_ref,
    key_ref,
    value_ref,
    keep_ref,
    line_keep_ref,
    keys_ref,
    values_ref,
):
    down_products(core_ref[0], hidden_ref[...], dense_ref[...].astype(F32), down_ref, own_ref, keep_ref, line_keep_ref)
    normed = rms_scale(tokens_ref[...], gain_ref[...]).astype(BF16)
    for weight_ref, target_ref in ((key_ref, keys_ref), (value_ref, values_ref)):
        target_ref[...] = lax.dot_general(
            normed, weight_ref[...], (((1,), (1,)), ((), ())), preferred_element_type=F32
        ).astype(BF16)


def combine_kernel(back_ref, combine_ref, line_ref, line_keep_ref, line_got_ref, send_ref):
    lines, seq_count, half = send_ref.shape
    token_total = lines * seq_count
    slot_total = back_ref.shape[0] * back_ref.shape[1]
    back = back_ref[...].reshape(slot_total, half)
    routed = jnp.dot(combine_ref[:, :slot_total], back, preferred_element_type=F32)
    routed += jnp.dot(combine_ref[:, slot_total:], back, preferred_element_type=F32)
    meta = line_ref[...].reshape(token_total, line_ref.shape[2])[:, half:].astype(F32)
    mix = meta[:, MIX_HI : MIX_HI + 1] + meta[:, MIX_LO : MIX_LO + 1]
    dense = line_keep_ref[...].astype(F32) + line_got_ref[...].astype(F32)
    send_ref[...] = (routed + mix * dense).astype(BF16).reshape(lines, seq_count, half)


def finish_kernel(residual_ref, parts_ref, out_ref):
    total = parts_ref[0].astype(F32)
    for n in range(1, parts_ref.shape[0]):
        total += parts_ref[n].astype(F32)
    out_ref[...] = (residual_ref[...].astype(F32) + total).astype(BF16)


def shards(
    tokens,
    lengths,
    attn_gain,
    w_query,
    w_key,
    w_value,
    head_bias,
    key_cache,
    value_cache,
    w_attn_out,
    ffn_gain,
    w_router,
    routes,
    w_dense_gate,
    w_dense_up,
    w_dense_down,
    dense_mix,
    w_expert_gate,
    w_expert_up,
    w_expert_down,
):
    seq_count, width = tokens.shape
    half = width // 2
    lines = lax.axis_size(LINE)
    places = lax.axis_size(PLANE)
    slot_total = places * seq_count
    token_total = lines * seq_count
    core = lax.axis_index("tp").astype(jnp.int32).reshape(1)
    line = lax.axis_index(LINE).astype(jnp.int32).reshape(1)
    cache_rows = seq_count * key_cache.shape[2]
    cache_len = key_cache.shape[3]
    attn_own = call(
        attend_kernel,
        jax.ShapeDtypeStruct((seq_count, width), BF16),
        0,
        (
            head_bias.reshape(1, -1),
            lengths.reshape(1, seq_count),
            tokens,
            attn_gain.reshape(1, width),
            w_query,
            key_cache.reshape(cache_rows, cache_len),
            value_cache.reshape(cache_rows, cache_len),
            w_attn_out,
        ),
        24,
        hbm_count=8,
        scratch=(
            pltpu.VMEM((1, head_bias.shape[0]), F32),
            pltpu.VMEM((1, seq_count), jnp.int32),
            pltpu.VMEM(tokens.shape, BF16),
            pltpu.VMEM((1, width), F32),
            pltpu.VMEM(w_query.shape, BF16),
            pltpu.VMEM((cache_rows, cache_len), BF16),
            pltpu.VMEM((cache_rows, cache_len), BF16),
            pltpu.VMEM(w_attn_out.shape, BF16),
            pltpu.SemaphoreType.DMA((11,)),
        ),
    )
    attn_other = lax.ppermute(attn_own, "tp", SWAP)
    line_send, residual = call(
        rows_kernel,
        (
            jax.ShapeDtypeStruct((lines, seq_count, half + 128), BF16),
            jax.ShapeDtypeStruct((seq_count, half), BF16),
        ),
        2,
        (
            core,
            line,
            tokens,
            attn_own,
            attn_other,
            ffn_gain.reshape(1, width),
            w_router,
            routes,
            w_dense_gate,
            w_dense_up,
            w_dense_down.T,
            dense_mix.reshape(1, width),
        ),
        8,
    )
    line_own = lax.all_to_all(line_send, LINE, 0, 0, tiled=True)
    line_other = lax.ppermute(line_own, "tp", SWAP)
    slot_send, combine = call(
        slots_kernel,
        (
            jax.ShapeDtypeStruct((places, seq_count, half + 96 * lines), BF16),
            jax.ShapeDtypeStruct((token_total, 2 * slot_total), BF16),
        ),
        1,
        (line, line_own),
        8,
    )
    slot_own = lax.all_to_all(slot_send, PLANE, 0, 0, tiled=True)
    slot_other = lax.ppermute(slot_own, "tp", SWAP)
    weights = (w_expert_gate[0], w_expert_up[0])
    hidden_shape = (slot_total, w_expert_gate.shape[2])
    sums = call(
        own_kernel,
        (jax.ShapeDtypeStruct(hidden_shape, F32),) * 2 + (jax.ShapeDtypeStruct((2, token_total, 128), F32),),
        1,
        (core, slot_own, line_own, *weights),
        8,
    )
    both_shape = (
        jax.ShapeDtypeStruct((slot_total, half), BF16),
        jax.ShapeDtypeStruct((token_total, half), BF16),
    )
    send, dense_send, hidden, dense = call(
        other_kernel,
        (*both_shape, jax.ShapeDtypeStruct(hidden_shape, BF16), jax.ShapeDtypeStruct((token_total, 128), BF16)),
        1,
        (core, *sums, slot_own, slot_other, line_other, *weights, w_expert_down[0]),
        12,
    )
    got = lax.ppermute(send, "tp", SWAP)
    dense_got = lax.ppermute(dense_send, "tp", SWAP)
    new_shape = jax.ShapeDtypeStruct((seq_count, w_key.shape[1]), BF16)
    keep, dense_keep, new_keys, new_values = call(
        keep_kernel,
        (*both_shape, new_shape, new_shape),
        1,
        (
            core,
            hidden,
            dense,
            slot_own,
            w_expert_down[0],
            tokens,
            attn_gain.reshape(1, width),
            w_key.T,
            w_value.T,
        ),
        8,
    )
    results = (keep.astype(F32) + got.astype(F32)).astype(BF16)
    results, dense_got = lax.optimization_barrier((results, dense_got))
    back = lax.all_to_all(results.reshape(places, seq_count, half), PLANE, 0, 0, tiled=True)
    partial = call(
        combine_kernel,
        jax.ShapeDtypeStruct((lines, seq_count, half), BF16),
        0,
        (back, combine, line_own, dense_keep, dense_got),
        8,
    )
    parts = lax.all_to_all(partial, LINE, 0, 0, tiled=True)
    layer_out = call(finish_kernel, jax.ShapeDtypeStruct((seq_count, half), BF16), 0, (residual, parts), 8)
    return (layer_out, new_keys, new_values)


def solution(mesh):
    finer = Mesh(mesh.devices.reshape(8, 4, 4, mesh.shape["tp"]), ("ep_0", "ep_1", "ep_2", "tp"))
    placed = (
        P(EP, None),
        P(EP),
        P(),
        P(None, "tp"),
        P(None, "tp"),
        P(None, "tp"),
        P("tp"),
        P(EP, "tp", None, None),
        P(EP, "tp", None, None),
        P("tp", None),
        P(),
        P(),
        P(EP, None),
        P(EP, "tp"),
        P(EP, "tp"),
        P("tp", EP),
        P(),
        P(EP, None, "tp"),
        P(EP, None, "tp"),
        P(EP, "tp", None),
    )
    return jax.shard_map(
        shards,
        mesh=finer,
        in_specs=placed,
        out_specs=(P(EP, "tp"), P(EP, "tp"), P(EP, "tp")),
        check_vma=False,
    )
```

```python
import jax
import jax.numpy as jnp
from jax import lax
from jax.experimental import pallas as pl
from jax.experimental.pallas import tpu as pltpu
from jax.sharding import Mesh
from jax.sharding import PartitionSpec as P

EP = ("ep_0", "ep_1", "ep_2")
LINE = "ep_0"
PLANE = ("ep_1", "ep_2")
SWAP = ((0, 1), (1, 0))
F32 = jnp.float32
BF16 = jnp.bfloat16

GATE_HI, GATE_LO, MIX_HI, MIX_LO, DENSE = 8, 16, 24, 25, 32


def rms_scale(values, gain):
    wide = values.astype(F32)
    return wide * lax.rsqrt(jnp.mean(wide * wide, axis=-1, keepdims=True) + 1e-06) * gain


def attend_kernel(
    bias_hbm,
    lengths_hbm,
    tokens_hbm,
    gain_hbm,
    query_hbm,
    key_hbm,
    value_hbm,
    out_hbm,
    partial_ref,
    bias_ref,
    lengths_ref,
    tokens_ref,
    gain_ref,
    query_buf,
    key_buf,
    value_buf,
    out_buf,
    sems,
):
    seq_count, width = tokens_ref.shape
    head_total = query_buf.shape[1]
    row_total, cache_len = key_buf.shape
    head_dim = row_total // seq_count
    heads = head_total // head_dim
    copies = []

    def fetch(source, target, pieces):
        size = source.shape[0] // pieces
        made = []
        for n in range(pieces):
            at = pl.ds(n * size, size)
            made.append(pltpu.make_async_copy(source.at[at, :], target.at[at, :], sems.at[len(copies)]))
            copies.append(made[-1])
        return made

    small_copies = [
        fetch(source, target, 1)[0]
        for source, target in (
            (tokens_hbm, tokens_ref),
            (gain_hbm, gain_ref),
            (bias_hbm, bias_ref),
            (lengths_hbm, lengths_ref),
        )
    ]
    query_copies = fetch(query_hbm, query_buf, 2)
    key_copies = fetch(key_hbm, key_buf, 2)
    value_copies = fetch(value_hbm, value_buf, 2)
    out_copies = fetch(out_hbm, out_buf, 1)
    for copy in copies:
        copy.start()

    for copy in small_copies:
        copy.wait()
    normed = rms_scale(tokens_ref[...], gain_ref[...]).astype(BF16)
    row = lax.broadcasted_iota(jnp.int32, (heads * seq_count, 1), 0)
    bias = jnp.zeros((heads * seq_count, 1), F32)
    for h in range(heads):
        bias = jnp.where(row // seq_count == h, bias_ref[:, h : h + 1], bias)
    lengths = jnp.zeros((seq_count, 1), jnp.int32)
    for n in range(seq_count):
        lengths = jnp.where(row[:seq_count] == n, lengths_ref[:, n : n + 1], lengths)
    lengths = jnp.concatenate([lengths] * heads, axis=0)
    lane = lax.broadcasted_iota(jnp.int32, (seq_count, 128), 1)
    low = lane < head_dim
    own = (
        lax.broadcasted_iota(jnp.int32, (seq_count, row_total), 1) // head_dim
        == lax.broadcasted_iota(jnp.int32, (seq_count, row_total), 0)
    )
    span = 256
    after_mask = (
        lax.broadcasted_iota(jnp.int32, (span, span), 0) > lax.broadcasted_iota(jnp.int32, (span, span), 1)
    ).astype(BF16)

    queries = jnp.zeros((seq_count, head_total), F32)
    piece = width // len(query_copies)
    for n, copy in enumerate(query_copies):
        copy.wait()
        at = slice(n * piece, (n + 1) * piece)
        queries += jnp.dot(normed[:, at], query_buf[at, :], preferred_element_type=F32)
    queries = queries.astype(BF16).astype(F32)
    spread = []
    for h in range(heads):
        tile = queries[:, h // 2 * 128 : h // 2 * 128 + 128]
        turned = pltpu.roll(tile, head_dim, 1)
        both = jnp.where(low, tile, turned) if h % 2 == 0 else jnp.where(low, turned, tile)
        wide = jnp.concatenate([both] * (row_total // 128), axis=1)
        spread.append(jnp.where(own, wide, 0.0).astype(BF16))
    spread = jnp.concatenate(spread, axis=0)

    scores = None
    piece = row_total // len(key_copies)
    for n, copy in enumerate(key_copies):
        copy.wait()
        at = slice(n * piece, (n + 1) * piece)
        part = jnp.dot(spread[:, at], key_buf[at, :], preferred_element_type=F32)
        scores = part if scores is None else scores + part
    later = jnp.zeros((heads * seq_count, 1), F32)
    sticks = []
    for block in reversed(range(cache_len // span)):
        score = scores[:, block * span : (block + 1) * span] * head_dim ** (-0.5) + bias
        position = lax.broadcasted_iota(jnp.int32, score.shape, 1) + block * span
        visible = position < lengths
        soft = jnp.log1p(jnp.exp(-jnp.abs(score)))
        log_keep = jnp.where(visible, -(jnp.maximum(score, 0.0) + soft), 0.0)
        high = log_keep.astype(BF16)
        rest = (log_keep - high.astype(F32)).astype(BF16)
        log_after = jnp.dot(high, after_mask, preferred_element_type=F32)
        log_after += jnp.dot(rest, after_mask, preferred_element_type=F32)
        weight = jnp.exp(jnp.minimum(score, 0.0) - soft + (log_after + later))
        sticks.append(jnp.where(visible, weight, 0.0).astype(BF16))
        later += jnp.sum(log_keep, axis=-1, keepdims=True)
    sticks = jnp.concatenate(sticks[::-1], axis=1)

    read = []
    piece = row_total // len(value_copies)
    for n, copy in enumerate(value_copies):
        copy.wait()
        read.append(
            lax.dot_general(
                sticks,
                value_buf[n * piece : (n + 1) * piece, :],
                (((1,), (1,)), ((), ())),
                preferred_element_type=F32,
            )
        )
    read = jnp.concatenate(read, axis=1)
    folded = []
    for h in range(heads):
        mine = jnp.where(own, read[h * seq_count : (h + 1) * seq_count], 0.0)
        tile = mine[:, :128]
        for n in range(1, row_total // 128):
            tile += mine[:, n * 128 : (n + 1) * 128]
        folded.append(tile + pltpu.roll(tile, head_dim, 1))
    heads_out = jnp.concatenate(
        [jnp.where(low, folded[h], folded[h + 1]) for h in range(0, heads, 2)], axis=1
    ).astype(BF16)
    for copy in out_copies:
        copy.wait()
    partial_ref[...] = jnp.dot(heads_out, out_buf[...], preferred_element_type=F32).astype(BF16)


def call(kernel, out_shape, smem_count, inputs, limit, hbm_count=0, scratch=()):
    in_specs = [pl.BlockSpec(memory_space=pltpu.SMEM)] * smem_count
    in_specs += [pl.BlockSpec(memory_space=pltpu.VMEM)] * (len(inputs) - smem_count - hbm_count)
    in_specs += [pl.BlockSpec(memory_space=pltpu.HBM)] * hbm_count
    held = [pltpu.with_memory_space_constraint(x, pltpu.HBM) for x in inputs[len(inputs) - hbm_count :]]
    return pl.pallas_call(
        kernel,
        out_shape=out_shape,
        in_specs=in_specs,
        out_specs=jax.tree.map(lambda _: pl.BlockSpec(memory_space=pltpu.VMEM), out_shape),
        scratch_shapes=scratch,
        compiler_params=pltpu.CompilerParams(vmem_limit_bytes=limit * 1024 * 1024),
    )(*inputs[: len(inputs) - hbm_count], *held)


def rows_kernel(
    core_ref,
    line_ref,
    tokens_ref,
    own_ref,
    other_ref,
    gain_ref,
    router_ref,
    routes_ref,
    gate_ref,
    up_ref,
    down_ref,
    mix_ref,
    send_ref,
    residual_ref,
):
    first_core = core_ref[0] == 0
    lines, seq_count, _ = send_ref.shape
    half = residual_ref.shape[1]
    attn = own_ref[...].astype(F32) + other_ref[...].astype(F32)
    residual = (tokens_ref[...].astype(F32) + attn).astype(BF16)
    normed = rms_scale(residual, gain_ref[...]).astype(BF16)
    residual_ref[...] = jnp.where(first_core, residual[:, :half], residual[:, half:])
    probs = jax.nn.sigmoid(jnp.dot(normed, router_ref[...], preferred_element_type=F32))
    mix = jax.nn.sigmoid(jnp.sum(normed.astype(F32) * mix_ref[...], axis=-1, keepdims=True))
    routes = routes_ref[...]
    lane = lax.broadcasted_iota(jnp.int32, probs.shape, 1)
    picked = [
        jnp.sum(jnp.where(lane == routes[:, k : k + 1], probs, 0.0), axis=-1, keepdims=True)
        for k in range(routes.shape[1])
    ]
    total = sum(picked[1:], picked[0])
    meta_lane = lax.broadcasted_iota(jnp.int32, (seq_count, 128), 1)
    meta = jnp.zeros((seq_count, 128), F32)

    def put(meta, at, value):
        return jnp.where(meta_lane == at, value, meta)

    for k, one in enumerate(picked):
        gate = one / total * 2.5
        high = gate.astype(BF16).astype(F32)
        meta = put(meta, k, routes[:, k : k + 1].astype(F32))
        meta = put(meta, GATE_HI + k, high)
        meta = put(meta, GATE_LO + k, gate - high)
    mix_high = mix.astype(BF16).astype(F32)
    meta = put(put(meta, MIX_HI, mix_high), MIX_LO, mix - mix_high)
    parts = [ref[...].astype(F32) for ref in (gate_ref, up_ref, down_ref)]
    part = parts[0].shape[1] // lines
    row = jnp.where(first_core, normed[:, :half], normed[:, half:])
    for line in range(lines):
        block = meta
        at = line * part
        for n, values in enumerate(parts):
            tile = values[:, at // 128 * 128 : at // 128 * 128 + 128]
            to = DENSE + n * part
            moved = pltpu.roll(tile, (to - at % 128) % 128, 1)
            inside = jnp.logical_and(meta_lane >= to, meta_lane < to + part)
            block = jnp.where(inside, moved, block)
        send_ref[line, :, :half] = row
        send_ref[line, :, half:] = block.astype(BF16)


def slots_kernel(line_ref, got_ref, send_ref, combine_ref):
    lines, seq_count, width = got_ref.shape
    places = send_ref.shape[0]
    half = width - 128
    token_total = lines * seq_count
    capacity = seq_count
    slot_total = places * capacity
    got = got_ref[...].reshape(token_total, width)
    meta = got[:, half:].astype(F32).T
    slot = lax.broadcasted_iota(jnp.int32, (slot_total, token_total), 0)
    token = lax.broadcasted_iota(jnp.int32, (slot_total, token_total), 1)
    expert = (line_ref[0] * places + slot // capacity).astype(F32)
    hit = jnp.zeros((slot_total, token_total), F32)
    gate = jnp.zeros((slot_total, token_total), F32)
    for k in range(6):
        same = meta[k : k + 1] == expert
        hit = jnp.where(same, 1.0, hit)
        gate = jnp.where(same, meta[GATE_HI + k : GATE_HI + k + 1] + meta[GATE_LO + k : GATE_LO + k + 1], gate)
    row = lax.broadcasted_iota(jnp.int32, (token_total, token_total), 0)
    column = lax.broadcasted_iota(jnp.int32, (token_total, token_total), 1)
    earlier = jnp.logical_and(row // seq_count == column // seq_count, row < column)
    rank = jnp.dot(hit.astype(BF16), earlier.astype(BF16), preferred_element_type=F32)
    per_source = capacity // lines
    here = jnp.logical_and(
        token // seq_count == slot % capacity // per_source,
        rank == (slot % per_source).astype(F32),
    )
    chosen = jnp.where(here, hit, 0.0)
    rows = jnp.dot(chosen.astype(BF16), got[:, :half], preferred_element_type=F32)
    send_ref[:, :, :half] = rows.astype(BF16).reshape(places, capacity, half)
    group = (lax.broadcasted_iota(jnp.int32, (seq_count, 128), 1)) // 32
    for n in range(3):
        for first in range(0, lines, 4):
            tile = jnp.zeros((seq_count, 128), F32)
            for k in range(4):
                block = got[(first + k) * seq_count : (first + k + 1) * seq_count, half:].astype(F32)
                moved = pltpu.roll(block, (k * 32 - DENSE - n * 32) % 128, 1)
                tile = jnp.where(group == k, moved, tile)
            at = half + (n * lines + first) * 32
            send_ref[:, :, at : at + 128] = jnp.broadcast_to(tile.astype(BF16)[None], (places, seq_count, 128))
    weights = jnp.where(here, gate * hit, 0.0).T
    high = weights.astype(BF16)
    combine_ref[:, :slot_total] = high
    combine_ref[:, slot_total:] = (weights - high.astype(F32)).astype(BF16)


def dense_weights(slots_ref, half, part, line):
    lanes = 32 * 8
    at = pl.multiple_of(half + part * lanes + line // 4 * 128, 128)
    return slots_ref[:, :, pl.ds(at, 128)].reshape(-1, 128)


def lane_group(shape):
    return lax.broadcasted_iota(jnp.int32, shape, 1) // 32


def half_products(side, slots_ref, width, gate_ref, up_ref):
    half = width // 2
    mine = pl.ds(pl.multiple_of(side * half, half), half)
    values = slots_ref[:, :, :half].reshape(-1, half)
    return tuple(jnp.dot(values, ref[mine, :], preferred_element_type=F32) for ref in (gate_ref, up_ref))


def dense_share(core, slots_ref, line_own_ref, line_other_ref):
    half = line_own_ref.shape[2] - 128
    block = half // 4
    group = lane_group((line_own_ref.shape[0] * line_own_ref.shape[1], 128))
    sums = []
    for part in range(2):
        total = jnp.zeros(group.shape, F32)
        for side, line_ref in ((core, line_own_ref), (1 - core, line_other_ref)):
            rows = line_ref[:, :, :half].reshape(-1, half)
            weights = dense_weights(slots_ref, half, part, side * 4)
            for k in range(4):
                product = jnp.dot(rows[:, k * block : (k + 1) * block], weights, preferred_element_type=F32)
                total += jnp.where(group == k, product, 0.0)
        total += pltpu.roll(total, 64, 1)
        sums.append(total + pltpu.roll(total, 32, 1))
    hidden = (jax.nn.silu(sums[0]) * sums[1]).astype(BF16).astype(F32)
    weights = dense_weights(slots_ref, half, 2, core * 4)
    return [
        lax.dot_general(
            jnp.where(group == k, hidden, 0.0).astype(BF16),
            weights,
            (((1,), (1,)), ((), ())),
            preferred_element_type=F32,
        )
        for k in range(4)
    ]


def own_kernel(
    core_ref,
    slots_ref,
    gate_ref,
    up_ref,
    tokens_ref,
    gain_ref,
    key_ref,
    value_ref,
    gate_out,
    up_out,
    keys_ref,
    values_ref,
):
    core = core_ref[0]
    gate_out[...], up_out[...] = half_products(core, slots_ref, gate_ref.shape[0], gate_ref, up_ref)
    normed = rms_scale(tokens_ref[...], gain_ref[...]).astype(BF16)
    for weight_ref, target_ref in ((key_ref, keys_ref), (value_ref, values_ref)):
        target_ref[...] = lax.dot_general(
            normed, weight_ref[...], (((1,), (1,)), ((), ())), preferred_element_type=F32
        ).astype(BF16)


def down_product(side, hidden, down_ref):
    half = down_ref.shape[1] // 2
    mine = pl.ds(pl.multiple_of(side * half, half), half)
    return jnp.dot(hidden, down_ref[:, mine], preferred_element_type=F32).astype(BF16)


def other_kernel(
    core_ref, gate_sum, up_sum, other_ref, line_other_ref, gate_ref, up_ref, down_ref, send_ref, hidden_ref
):
    del line_other_ref
    side = 1 - core_ref[0]
    gate, up = half_products(side, other_ref, gate_ref.shape[0], gate_ref, up_ref)
    hidden = (jax.nn.silu(gate_sum[...] + gate) * (up_sum[...] + up)).astype(BF16)
    hidden_ref[...] = hidden
    send_ref[...] = down_product(side, hidden, down_ref)


def keep_kernel(
    core_ref, hidden_ref, down_ref, own_ref, other_ref, line_own_ref, line_other_ref, keep_ref, dense_out
):
    core = core_ref[0]
    keep_ref[...] = down_product(core, hidden_ref[...], down_ref)
    block = dense_out.shape[1] // 4
    shares = [dense_share(core, ref, line_own_ref, line_other_ref) for ref in (own_ref, other_ref)]
    for k, (own, other) in enumerate(zip(*shares, strict=True)):
        dense_out[:, k * block : (k + 1) * block] = own + other


def combine_kernel(back_ref, combine_ref, line_ref, dense_ref, send_ref):
    lines, seq_count, half = send_ref.shape
    token_total = lines * seq_count
    slot_total = back_ref.shape[0] * back_ref.shape[1]
    back = back_ref[...].reshape(slot_total, half)
    routed = jnp.dot(combine_ref[:, :slot_total], back, preferred_element_type=F32)
    routed += jnp.dot(combine_ref[:, slot_total:], back, preferred_element_type=F32)
    meta = line_ref[...].reshape(token_total, line_ref.shape[2])[:, half:].astype(F32)
    mix = meta[:, MIX_HI : MIX_HI + 1] + meta[:, MIX_LO : MIX_LO + 1]
    send_ref[...] = (routed + mix * dense_ref[...]).astype(BF16).reshape(lines, seq_count, half)


def finish_kernel(residual_ref, parts_ref, out_ref):
    total = parts_ref[0].astype(F32)
    for n in range(1, parts_ref.shape[0]):
        total += parts_ref[n].astype(F32)
    out_ref[...] = (residual_ref[...].astype(F32) + total).astype(BF16)


def shards(
    tokens,
    lengths,
    attn_gain,
    w_query,
    w_key,
    w_value,
    head_bias,
    key_cache,
    value_cache,
    w_attn_out,
    ffn_gain,
    w_router,
    routes,
    w_dense_gate,
    w_dense_up,
    w_dense_down,
    dense_mix,
    w_expert_gate,
    w_expert_up,
    w_expert_down,
):
    seq_count, width = tokens.shape
    half = width // 2
    lines = lax.axis_size(LINE)
    places = lax.axis_size(PLANE)
    slot_total = places * seq_count
    token_total = lines * seq_count
    core = lax.axis_index("tp").astype(jnp.int32).reshape(1)
    line = lax.axis_index(LINE).astype(jnp.int32).reshape(1)
    cache_rows = seq_count * key_cache.shape[2]
    cache_len = key_cache.shape[3]
    attn_own = call(
        attend_kernel,
        jax.ShapeDtypeStruct((seq_count, width), BF16),
        0,
        (
            head_bias.reshape(1, -1),
            lengths.reshape(1, seq_count),
            tokens,
            attn_gain.reshape(1, width),
            w_query,
            key_cache.reshape(cache_rows, cache_len),
            value_cache.reshape(cache_rows, cache_len),
            w_attn_out,
        ),
        24,
        hbm_count=8,
        scratch=(
            pltpu.VMEM((1, head_bias.shape[0]), F32),
            pltpu.VMEM((1, seq_count), jnp.int32),
            pltpu.VMEM(tokens.shape, BF16),
            pltpu.VMEM((1, width), F32),
            pltpu.VMEM(w_query.shape, BF16),
            pltpu.VMEM((cache_rows, cache_len), BF16),
            pltpu.VMEM((cache_rows, cache_len), BF16),
            pltpu.VMEM(w_attn_out.shape, BF16),
            pltpu.SemaphoreType.DMA((11,)),
        ),
    )
    attn_other = lax.ppermute(attn_own, "tp", SWAP)
    line_send, residual = call(
        rows_kernel,
        (
            jax.ShapeDtypeStruct((lines, seq_count, half + 128), BF16),
            jax.ShapeDtypeStruct((seq_count, half), BF16),
        ),
        2,
        (
            core,
            line,
            tokens,
            attn_own,
            attn_other,
            ffn_gain.reshape(1, width),
            w_router,
            routes,
            w_dense_gate,
            w_dense_up,
            w_dense_down.T,
            dense_mix.reshape(1, width),
        ),
        8,
    )
    line_own = lax.all_to_all(line_send, LINE, 0, 0, tiled=True)
    line_other = lax.ppermute(line_own, "tp", SWAP)
    slot_send, combine = call(
        slots_kernel,
        (
            jax.ShapeDtypeStruct((places, seq_count, half + 96 * lines), BF16),
            jax.ShapeDtypeStruct((token_total, 2 * slot_total), BF16),
        ),
        1,
        (line, line_own),
        8,
    )
    slot_own = lax.all_to_all(slot_send, PLANE, 0, 0, tiled=True)
    slot_other = lax.ppermute(slot_own, "tp", SWAP)
    weights = (w_expert_gate[0], w_expert_up[0])
    hidden_shape = (slot_total, w_expert_gate.shape[2])
    hidden_shape = (slot_total, w_expert_gate.shape[2])
    new_shape = jax.ShapeDtypeStruct((seq_count, w_key.shape[1]), BF16)
    dense_shape = jax.ShapeDtypeStruct((token_total, half), F32)
    gate_sum, up_sum, new_keys, new_values = call(
        own_kernel,
        (*(jax.ShapeDtypeStruct(hidden_shape, F32),) * 2, new_shape, new_shape),
        1,
        (core, slot_own, *weights, tokens, attn_gain.reshape(1, width), w_key.T, w_value.T),
        8,
    )
    result_shape = jax.ShapeDtypeStruct((slot_total, half), BF16)
    send, hidden = call(
        other_kernel,
        (result_shape, jax.ShapeDtypeStruct(hidden_shape, BF16)),
        1,
        (core, gate_sum, up_sum, slot_other, line_other, *weights, w_expert_down[0]),
        12,
    )
    got = lax.ppermute(send, "tp", SWAP)
    keep, dense = call(
        keep_kernel,
        (result_shape, dense_shape),
        1,
        (core, hidden, w_expert_down[0], slot_own, slot_other, line_own, line_other),
        12,
    )
    results = (keep.astype(F32) + got.astype(F32)).astype(BF16)
    back = lax.all_to_all(results.reshape(places, seq_count, half), PLANE, 0, 0, tiled=True)
    partial = call(
        combine_kernel,
        jax.ShapeDtypeStruct((lines, seq_count, half), BF16),
        0,
        (back, combine, line_own, dense),
        8,
    )
    parts = lax.all_to_all(partial, LINE, 0, 0, tiled=True)
    layer_out = call(finish_kernel, jax.ShapeDtypeStruct((seq_count, half), BF16), 0, (residual, parts), 8)
    return (layer_out, new_keys, new_values)


def solution(mesh):
    finer = Mesh(mesh.devices.reshape(8, 4, 4, mesh.shape["tp"]), ("ep_0", "ep_1", "ep_2", "tp"))
    placed = (
        P(EP, None),
        P(EP),
        P(),
        P(None, "tp"),
        P(None, "tp"),
        P(None, "tp"),
        P("tp"),
        P(EP, "tp", None, None),
        P(EP, "tp", None, None),
        P("tp", None),
        P(),
        P(),
        P(EP, None),
        P(EP, "tp"),
        P(EP, "tp"),
        P("tp", EP),
        P(),
        P(EP, None, "tp"),
        P(EP, None, "tp"),
        P(EP, "tp", None),
    )
    return jax.shard_map(
        shards,
        mesh=finer,
        in_specs=placed,
        out_specs=(P(EP, "tp"), P(EP, "tp"), P(EP, "tp")),
        check_vma=False,
    )
```

```python
import jax
import jax.numpy as jnp
from jax import lax
from jax.experimental import pallas as pl
from jax.experimental.pallas import tpu as pltpu
from jax.sharding import Mesh
from jax.sharding import PartitionSpec as P

EP = ("ep_0", "ep_1", "ep_2")
LINE = "ep_0"
PLANE = ("ep_1", "ep_2")
SWAP = ((0, 1), (1, 0))
F32 = jnp.float32
BF16 = jnp.bfloat16

GATE_HI, GATE_LO, MIX_HI, MIX_LO, DENSE = 8, 16, 24, 25, 32


def rms_scale(values, gain):
    wide = values.astype(F32)
    return wide * lax.rsqrt(jnp.mean(wide * wide, axis=-1, keepdims=True) + 1e-06) * gain


def attend_kernel(
    bias_hbm,
    lengths_hbm,
    tokens_hbm,
    gain_hbm,
    query_hbm,
    key_hbm,
    value_hbm,
    out_hbm,
    router_hbm,
    partial_ref,
    router_ref,
    bias_ref,
    lengths_ref,
    tokens_ref,
    gain_ref,
    query_buf,
    key_buf,
    value_buf,
    out_buf,
    sems,
):
    seq_count, width = tokens_ref.shape
    head_total = query_buf.shape[1]
    row_total, cache_len = key_buf.shape
    head_dim = row_total // seq_count
    heads = head_total // head_dim
    copies = []

    def fetch(source, target, pieces):
        size = source.shape[0] // pieces
        made = []
        for n in range(pieces):
            at = pl.ds(n * size, size)
            made.append(pltpu.make_async_copy(source.at[at, :], target.at[at, :], sems.at[len(copies)]))
            copies.append(made[-1])
        return made

    small_copies = [
        fetch(source, target, 1)[0]
        for source, target in (
            (tokens_hbm, tokens_ref),
            (gain_hbm, gain_ref),
            (bias_hbm, bias_ref),
            (lengths_hbm, lengths_ref),
        )
    ]
    query_copies = fetch(query_hbm, query_buf, 4)
    key_copies = fetch(key_hbm, key_buf, 2)
    value_copies = fetch(value_hbm, value_buf, 2)
    out_copies = fetch(out_hbm, out_buf, 1)
    router_copies = fetch(router_hbm, router_ref, 1)
    for copy in copies:
        copy.start()

    for copy in small_copies:
        copy.wait()
    normed = rms_scale(tokens_ref[...], gain_ref[...]).astype(BF16)
    parts = len(key_copies)
    part = seq_count // parts
    part_rows = row_total // parts
    row = lax.broadcasted_iota(jnp.int32, (heads * part, 1), 0)
    bias = jnp.zeros((heads * part, 1), F32)
    for h in range(heads):
        bias = jnp.where(row // part == h, bias_ref[:, h : h + 1], bias)
    low = lax.broadcasted_iota(jnp.int32, (part, 128), 1) < head_dim
    own = (
        lax.broadcasted_iota(jnp.int32, (part, part_rows), 1) // head_dim
        == lax.broadcasted_iota(jnp.int32, (part, part_rows), 0)
    )
    span = 256
    after_mask = (
        lax.broadcasted_iota(jnp.int32, (span, span), 0) > lax.broadcasted_iota(jnp.int32, (span, span), 1)
    ).astype(BF16)
    lengths = []
    for n in range(parts):
        column = jnp.zeros((part, 1), jnp.int32)
        for k in range(part):
            at = n * part + k
            column = jnp.where(row[:part] == k, lengths_ref[:, at : at + 1], column)
        lengths.append(jnp.concatenate([column] * heads, axis=0))

    queries = jnp.zeros((seq_count, head_total), F32)
    piece = width // len(query_copies)
    for n, copy in enumerate(query_copies):
        copy.wait()
        at = slice(n * piece, (n + 1) * piece)
        queries += jnp.dot(normed[:, at], query_buf[at, :], preferred_element_type=F32)
    queries = queries.astype(BF16).astype(F32)

    def spread(n):
        out = []
        for h in range(heads):
            tile = queries[n * part : (n + 1) * part, h // 2 * 128 : h // 2 * 128 + 128]
            turned = pltpu.roll(tile, head_dim, 1)
            both = jnp.where(low, tile, turned) if h % 2 == 0 else jnp.where(low, turned, tile)
            out.append(jnp.where(own, jnp.concatenate([both] * (part_rows // 128), axis=1), 0.0))
        return jnp.concatenate(out, axis=0).astype(BF16)

    def stick(scores, lengths):
        later = jnp.zeros((heads * part, 1), F32)
        out = []
        for block in reversed(range(cache_len // span)):
            score = scores[:, block * span : (block + 1) * span] * head_dim ** (-0.5) + bias
            position = lax.broadcasted_iota(jnp.int32, score.shape, 1) + block * span
            visible = position < lengths
            soft = jnp.log1p(jnp.exp(-jnp.abs(score)))
            log_keep = jnp.where(visible, -(jnp.maximum(score, 0.0) + soft), 0.0)
            high = log_keep.astype(BF16)
            rest = (log_keep - high.astype(F32)).astype(BF16)
            log_after = jnp.dot(high, after_mask, preferred_element_type=F32)
            log_after += jnp.dot(rest, after_mask, preferred_element_type=F32)
            weight = jnp.exp(jnp.minimum(score, 0.0) - soft + (log_after + later))
            out.append(jnp.where(visible, weight, 0.0).astype(BF16))
            later += jnp.sum(log_keep, axis=-1, keepdims=True)
        return jnp.concatenate(out[::-1], axis=1)

    spreads = [spread(n) for n in range(parts)]
    sticks = []
    for n, copy in enumerate(key_copies):
        copy.wait()
        keys = key_buf[n * part_rows : (n + 1) * part_rows, :]
        sticks.append(stick(jnp.dot(spreads[n], keys, preferred_element_type=F32), lengths[n]))
    heads_out = []
    for n, copy in enumerate(value_copies):
        copy.wait()
        values = value_buf[n * part_rows : (n + 1) * part_rows, :]
        read = lax.dot_general(sticks[n], values, (((1,), (1,)), ((), ())), preferred_element_type=F32)
        folded = []
        for h in range(heads):
            mine = jnp.where(own, read[h * part : (h + 1) * part], 0.0)
            tile = mine[:, :128]
            for k in range(1, part_rows // 128):
                tile += mine[:, k * 128 : (k + 1) * 128]
            folded.append(tile + pltpu.roll(tile, head_dim, 1))
        heads_out.append(
            jnp.concatenate([jnp.where(low, folded[h], folded[h + 1]) for h in range(0, heads, 2)], axis=1)
        )
    heads_out = jnp.concatenate(heads_out, axis=0).astype(BF16)
    for copy in out_copies:
        copy.wait()
    partial_ref[...] = jnp.dot(heads_out, out_buf[...], preferred_element_type=F32).astype(BF16)
    for copy in router_copies:
        copy.wait()


def call(kernel, out_shape, smem_count, inputs, limit, hbm_count=0, scratch=()):
    in_specs = [pl.BlockSpec(memory_space=pltpu.SMEM)] * smem_count
    in_specs += [pl.BlockSpec(memory_space=pltpu.VMEM)] * (len(inputs) - smem_count - hbm_count)
    in_specs += [pl.BlockSpec(memory_space=pltpu.HBM)] * hbm_count
    held = [pltpu.with_memory_space_constraint(x, pltpu.HBM) for x in inputs[len(inputs) - hbm_count :]]
    return pl.pallas_call(
        kernel,
        out_shape=out_shape,
        in_specs=in_specs,
        out_specs=jax.tree.map(lambda _: pl.BlockSpec(memory_space=pltpu.VMEM), out_shape),
        scratch_shapes=scratch,
        compiler_params=pltpu.CompilerParams(vmem_limit_bytes=limit * 1024 * 1024),
    )(*inputs[: len(inputs) - hbm_count], *held)


def rows_kernel(
    core_ref,
    line_ref,
    tokens_ref,
    own_ref,
    other_ref,
    gain_ref,
    router_ref,
    routes_ref,
    gate_ref,
    up_ref,
    down_ref,
    mix_ref,
    send_ref,
    residual_ref,
):
    first_core = core_ref[0] == 0
    lines, seq_count, _ = send_ref.shape
    half = residual_ref.shape[1]
    attn = own_ref[...].astype(F32) + other_ref[...].astype(F32)
    residual = (tokens_ref[...].astype(F32) + attn).astype(BF16)
    normed = rms_scale(residual, gain_ref[...]).astype(BF16)
    residual_ref[...] = jnp.where(first_core, residual[:, :half], residual[:, half:])
    probs = jax.nn.sigmoid(jnp.dot(normed, router_ref[...], preferred_element_type=F32))
    mix = jax.nn.sigmoid(jnp.sum(normed.astype(F32) * mix_ref[...], axis=-1, keepdims=True))
    routes = routes_ref[...]
    lane = lax.broadcasted_iota(jnp.int32, probs.shape, 1)
    picked = [
        jnp.sum(jnp.where(lane == routes[:, k : k + 1], probs, 0.0), axis=-1, keepdims=True)
        for k in range(routes.shape[1])
    ]
    total = sum(picked[1:], picked[0])
    meta_lane = lax.broadcasted_iota(jnp.int32, (seq_count, 128), 1)
    meta = jnp.zeros((seq_count, 128), F32)

    def put(meta, at, value):
        return jnp.where(meta_lane == at, value, meta)

    for k, one in enumerate(picked):
        gate = one / total * 2.5
        high = gate.astype(BF16).astype(F32)
        meta = put(meta, k, routes[:, k : k + 1].astype(F32))
        meta = put(meta, GATE_HI + k, high)
        meta = put(meta, GATE_LO + k, gate - high)
    mix_high = mix.astype(BF16).astype(F32)
    meta = put(put(meta, MIX_HI, mix_high), MIX_LO, mix - mix_high)
    parts = [ref[...].astype(F32) for ref in (gate_ref, up_ref, down_ref)]
    part = parts[0].shape[1] // lines
    row = jnp.where(first_core, normed[:, :half], normed[:, half:])
    for line in range(lines):
        block = meta
        at = line * part
        for n, values in enumerate(parts):
            tile = values[:, at // 128 * 128 : at // 128 * 128 + 128]
            to = DENSE + n * part
            moved = pltpu.roll(tile, (to - at % 128) % 128, 1)
            inside = jnp.logical_and(meta_lane >= to, meta_lane < to + part)
            block = jnp.where(inside, moved, block)
        send_ref[line, :, :half] = row
        send_ref[line, :, half:] = block.astype(BF16)


def slots_kernel(line_ref, got_ref, send_ref, combine_ref):
    lines, seq_count, width = got_ref.shape
    places = send_ref.shape[0]
    half = width - 128
    token_total = lines * seq_count
    capacity = seq_count
    slot_total = places * capacity
    got = got_ref[...].reshape(token_total, width)
    meta = got[:, half:].astype(F32).T
    slot = lax.broadcasted_iota(jnp.int32, (slot_total, token_total), 0)
    token = lax.broadcasted_iota(jnp.int32, (slot_total, token_total), 1)
    expert = (line_ref[0] * places + slot // capacity).astype(F32)
    hit = jnp.zeros((slot_total, token_total), F32)
    gate = jnp.zeros((slot_total, token_total), F32)
    for k in range(6):
        same = meta[k : k + 1] == expert
        hit = jnp.where(same, 1.0, hit)
        gate = jnp.where(same, meta[GATE_HI + k : GATE_HI + k + 1] + meta[GATE_LO + k : GATE_LO + k + 1], gate)
    row = lax.broadcasted_iota(jnp.int32, (token_total, token_total), 0)
    column = lax.broadcasted_iota(jnp.int32, (token_total, token_total), 1)
    earlier = jnp.logical_and(row // seq_count == column // seq_count, row < column)
    rank = jnp.dot(hit.astype(BF16), earlier.astype(BF16), preferred_element_type=F32)
    per_source = capacity // lines
    here = jnp.logical_and(
        token // seq_count == slot % capacity // per_source,
        rank == (slot % per_source).astype(F32),
    )
    chosen = jnp.where(here, hit, 0.0)
    rows = jnp.dot(chosen.astype(BF16), got[:, :half], preferred_element_type=F32)
    send_ref[:, :, :half] = rows.astype(BF16).reshape(places, capacity, half)
    group = (lax.broadcasted_iota(jnp.int32, (seq_count, 128), 1)) // 32
    for n in range(3):
        for first in range(0, lines, 4):
            tile = jnp.zeros((seq_count, 128), F32)
            for k in range(4):
                block = got[(first + k) * seq_count : (first + k + 1) * seq_count, half:].astype(F32)
                moved = pltpu.roll(block, (k * 32 - DENSE - n * 32) % 128, 1)
                tile = jnp.where(group == k, moved, tile)
            at = half + (n * lines + first) * 32
            send_ref[:, :, at : at + 128] = jnp.broadcast_to(tile.astype(BF16)[None], (places, seq_count, 128))
    weights = jnp.where(here, gate * hit, 0.0).T
    high = weights.astype(BF16)
    combine_ref[:, :slot_total] = high
    combine_ref[:, slot_total:] = (weights - high.astype(F32)).astype(BF16)


def dense_weights(slots_ref, half, part, line):
    lanes = 32 * 8
    at = pl.multiple_of(half + part * lanes + line // 4 * 128, 128)
    return slots_ref[:, :, pl.ds(at, 128)].reshape(-1, 128)


def lane_group(shape):
    return lax.broadcasted_iota(jnp.int32, shape, 1) // 32


def half_products(side, slots_ref, width, gate_ref, up_ref):
    half = width // 2
    mine = pl.ds(pl.multiple_of(side * half, half), half)
    values = slots_ref[:, :, :half].reshape(-1, half)
    return tuple(jnp.dot(values, ref[mine, :], preferred_element_type=F32) for ref in (gate_ref, up_ref))


def dense_share(core, slots_ref, line_own_ref, line_other_ref):
    half = line_own_ref.shape[2] - 128
    block = half // 4
    group = lane_group((line_own_ref.shape[0] * line_own_ref.shape[1], 128))
    sums = []
    for part in range(2):
        total = jnp.zeros(group.shape, F32)
        for side, line_ref in ((core, line_own_ref), (1 - core, line_other_ref)):
            rows = line_ref[:, :, :half].reshape(-1, half)
            weights = dense_weights(slots_ref, half, part, side * 4)
            for k in range(4):
                product = jnp.dot(rows[:, k * block : (k + 1) * block], weights, preferred_element_type=F32)
                total += jnp.where(group == k, product, 0.0)
        total += pltpu.roll(total, 64, 1)
        sums.append(total + pltpu.roll(total, 32, 1))
    hidden = (jax.nn.silu(sums[0]) * sums[1]).astype(BF16).astype(F32)
    weights = dense_weights(slots_ref, half, 2, core * 4)
    return [
        lax.dot_general(
            jnp.where(group == k, hidden, 0.0).astype(BF16),
            weights,
            (((1,), (1,)), ((), ())),
            preferred_element_type=F32,
        )
        for k in range(4)
    ]


def own_kernel(
    core_ref,
    slots_ref,
    gate_ref,
    up_ref,
    tokens_ref,
    gain_ref,
    key_ref,
    value_ref,
    gate_out,
    up_out,
    keys_ref,
    values_ref,
):
    core = core_ref[0]
    gate_out[...], up_out[...] = half_products(core, slots_ref, gate_ref.shape[0], gate_ref, up_ref)
    normed = rms_scale(tokens_ref[...], gain_ref[...]).astype(BF16)
    for weight_ref, target_ref in ((key_ref, keys_ref), (value_ref, values_ref)):
        target_ref[...] = lax.dot_general(
            normed, weight_ref[...], (((1,), (1,)), ((), ())), preferred_element_type=F32
        ).astype(BF16)


def down_product(side, hidden, down_ref):
    half = down_ref.shape[1] // 2
    mine = pl.ds(pl.multiple_of(side * half, half), half)
    return jnp.dot(hidden, down_ref[:, mine], preferred_element_type=F32).astype(BF16)


def other_kernel(
    core_ref, gate_sum, up_sum, other_ref, line_other_ref, gate_ref, up_ref, down_ref, send_ref, hidden_ref
):
    del line_other_ref
    side = 1 - core_ref[0]
    gate, up = half_products(side, other_ref, gate_ref.shape[0], gate_ref, up_ref)
    hidden = (jax.nn.silu(gate_sum[...] + gate) * (up_sum[...] + up)).astype(BF16)
    hidden_ref[...] = hidden
    send_ref[...] = down_product(side, hidden, down_ref)


def keep_kernel(
    core_ref, hidden_ref, down_ref, own_ref, other_ref, line_own_ref, line_other_ref, keep_ref, dense_out
):
    core = core_ref[0]
    keep_ref[...] = down_product(core, hidden_ref[...], down_ref)
    block = dense_out.shape[1] // 4
    shares = [dense_share(core, ref, line_own_ref, line_other_ref) for ref in (own_ref, other_ref)]
    for k, (own, other) in enumerate(zip(*shares, strict=True)):
        dense_out[:, k * block : (k + 1) * block] = own + other


def combine_kernel(back_ref, combine_ref, line_ref, dense_ref, send_ref):
    lines, seq_count, half = send_ref.shape
    token_total = lines * seq_count
    slot_total = back_ref.shape[0] * back_ref.shape[1]
    back = back_ref[...].reshape(slot_total, half)
    routed = jnp.dot(combine_ref[:, :slot_total], back, preferred_element_type=F32)
    routed += jnp.dot(combine_ref[:, slot_total:], back, preferred_element_type=F32)
    meta = line_ref[...].reshape(token_total, line_ref.shape[2])[:, half:].astype(F32)
    mix = meta[:, MIX_HI : MIX_HI + 1] + meta[:, MIX_LO : MIX_LO + 1]
    send_ref[...] = (routed + mix * dense_ref[...]).astype(BF16).reshape(lines, seq_count, half)


def finish_kernel(residual_ref, parts_ref, out_ref):
    total = parts_ref[0].astype(F32)
    for n in range(1, parts_ref.shape[0]):
        total += parts_ref[n].astype(F32)
    out_ref[...] = (residual_ref[...].astype(F32) + total).astype(BF16)


def shards(
    tokens,
    lengths,
    attn_gain,
    w_query,
    w_key,
    w_value,
    head_bias,
    key_cache,
    value_cache,
    w_attn_out,
    ffn_gain,
    w_router,
    routes,
    w_dense_gate,
    w_dense_up,
    w_dense_down,
    dense_mix,
    w_expert_gate,
    w_expert_up,
    w_expert_down,
):
    seq_count, width = tokens.shape
    half = width // 2
    lines = lax.axis_size(LINE)
    places = lax.axis_size(PLANE)
    slot_total = places * seq_count
    token_total = lines * seq_count
    core = lax.axis_index("tp").astype(jnp.int32).reshape(1)
    line = lax.axis_index(LINE).astype(jnp.int32).reshape(1)
    cache_rows = seq_count * key_cache.shape[2]
    cache_len = key_cache.shape[3]
    attn_own, router = call(
        attend_kernel,
        (jax.ShapeDtypeStruct((seq_count, width), BF16), jax.ShapeDtypeStruct(w_router.shape, BF16)),
        0,
        (
            head_bias.reshape(1, -1),
            lengths.reshape(1, seq_count),
            tokens,
            attn_gain.reshape(1, width),
            w_query,
            key_cache.reshape(cache_rows, cache_len),
            value_cache.reshape(cache_rows, cache_len),
            w_attn_out,
            w_router,
        ),
        24,
        hbm_count=9,
        scratch=(
            pltpu.VMEM((1, head_bias.shape[0]), F32),
            pltpu.VMEM((1, seq_count), jnp.int32),
            pltpu.VMEM(tokens.shape, BF16),
            pltpu.VMEM((1, width), F32),
            pltpu.VMEM(w_query.shape, BF16),
            pltpu.VMEM((cache_rows, cache_len), BF16),
            pltpu.VMEM((cache_rows, cache_len), BF16),
            pltpu.VMEM(w_attn_out.shape, BF16),
            pltpu.SemaphoreType.DMA((14,)),
        ),
    )
    attn_other = lax.ppermute(attn_own, "tp", SWAP)
    line_send, residual = call(
        rows_kernel,
        (
            jax.ShapeDtypeStruct((lines, seq_count, half + 128), BF16),
            jax.ShapeDtypeStruct((seq_count, half), BF16),
        ),
        2,
        (
            core,
            line,
            tokens,
            attn_own,
            attn_other,
            ffn_gain.reshape(1, width),
            router,
            routes,
            w_dense_gate,
            w_dense_up,
            w_dense_down.T,
            dense_mix.reshape(1, width),
        ),
        8,
    )
    line_own = lax.all_to_all(line_send, LINE, 0, 0, tiled=True)
    line_other = lax.ppermute(line_own, "tp", SWAP)
    slot_send, combine = call(
        slots_kernel,
        (
            jax.ShapeDtypeStruct((places, seq_count, half + 96 * lines), BF16),
            jax.ShapeDtypeStruct((token_total, 2 * slot_total), BF16),
        ),
        1,
        (line, line_own),
        8,
    )
    slot_own = lax.all_to_all(slot_send, PLANE, 0, 0, tiled=True)
    slot_other = lax.ppermute(slot_own, "tp", SWAP)
    weights = (w_expert_gate[0], w_expert_up[0])
    hidden_shape = (slot_total, w_expert_gate.shape[2])
    hidden_shape = (slot_total, w_expert_gate.shape[2])
    new_shape = jax.ShapeDtypeStruct((seq_count, w_key.shape[1]), BF16)
    dense_shape = jax.ShapeDtypeStruct((token_total, half), F32)
    gate_sum, up_sum, new_keys, new_values = call(
        own_kernel,
        (*(jax.ShapeDtypeStruct(hidden_shape, F32),) * 2, new_shape, new_shape),
        1,
        (core, slot_own, *weights, tokens, attn_gain.reshape(1, width), w_key.T, w_value.T),
        8,
    )
    result_shape = jax.ShapeDtypeStruct((slot_total, half), BF16)
    send, hidden = call(
        other_kernel,
        (result_shape, jax.ShapeDtypeStruct(hidden_shape, BF16)),
        1,
        (core, gate_sum, up_sum, slot_other, line_other, *weights, w_expert_down[0]),
        12,
    )
    got = lax.ppermute(send, "tp", SWAP)
    keep, dense = call(
        keep_kernel,
        (result_shape, dense_shape),
        1,
        (core, hidden, w_expert_down[0], slot_own, slot_other, line_own, line_other),
        12,
    )
    results = (keep.astype(F32) + got.astype(F32)).astype(BF16)
    back = lax.all_to_all(results.reshape(places, seq_count, half), PLANE, 0, 0, tiled=True)
    partial = call(
        combine_kernel,
        jax.ShapeDtypeStruct((lines, seq_count, half), BF16),
        0,
        (back, combine, line_own, dense),
        8,
    )
    parts = lax.all_to_all(partial, LINE, 0, 0, tiled=True)
    layer_out = call(finish_kernel, jax.ShapeDtypeStruct((seq_count, half), BF16), 0, (residual, parts), 8)
    return (layer_out, new_keys, new_values)


def solution(mesh):
    finer = Mesh(mesh.devices.reshape(8, 4, 4, mesh.shape["tp"]), ("ep_0", "ep_1", "ep_2", "tp"))
    placed = (
        P(EP, None),
        P(EP),
        P(),
        P(None, "tp"),
        P(None, "tp"),
        P(None, "tp"),
        P("tp"),
        P(EP, "tp", None, None),
        P(EP, "tp", None, None),
        P("tp", None),
        P(),
        P(),
        P(EP, None),
        P(EP, "tp"),
        P(EP, "tp"),
        P("tp", EP),
        P(),
        P(EP, None, "tp"),
        P(EP, None, "tp"),
        P(EP, "tp", None),
    )
    return jax.shard_map(
        shards,
        mesh=finer,
        in_specs=placed,
        out_specs=(P(EP, "tp"), P(EP, "tp"), P(EP, "tp")),
        check_vma=False,
    )
```

```python
import jax
import jax.numpy as jnp
from jax import lax
from jax.experimental import pallas as pl
from jax.experimental.pallas import tpu as pltpu
from jax.sharding import Mesh
from jax.sharding import PartitionSpec as P

EP = ("ep_0", "ep_1", "ep_2")
LINE = "ep_0"
PLANE = ("ep_1", "ep_2")
SWAP = ((0, 1), (1, 0))
F32 = jnp.float32
BF16 = jnp.bfloat16

GATE_HI, GATE_LO, MIX_HI, MIX_LO, DENSE = 8, 16, 24, 25, 32


def rms_scale(values, gain):
    wide = values.astype(F32)
    return wide * lax.rsqrt(jnp.mean(wide * wide, axis=-1, keepdims=True) + 1e-06) * gain


def attend_kernel(
    bias_hbm,
    lengths_hbm,
    tokens_hbm,
    gain_hbm,
    query_hbm,
    key_hbm,
    value_hbm,
    out_hbm,
    router_hbm,
    partial_ref,
    router_ref,
    bias_ref,
    lengths_ref,
    tokens_ref,
    gain_ref,
    query_buf,
    key_buf,
    value_buf,
    out_buf,
    sems,
):
    seq_count, width = tokens_ref.shape
    head_total = query_buf.shape[1]
    row_total, cache_len = key_buf.shape
    head_dim = row_total // seq_count
    heads = head_total // head_dim
    copies = []

    def fetch(source, target, pieces):
        size = source.shape[0] // pieces
        made = []
        for n in range(pieces):
            at = pl.ds(n * size, size)
            made.append(pltpu.make_async_copy(source.at[at, :], target.at[at, :], sems.at[len(copies)]))
            copies.append(made[-1])
        return made

    small_copies = [
        fetch(source, target, 1)[0]
        for source, target in (
            (tokens_hbm, tokens_ref),
            (gain_hbm, gain_ref),
            (bias_hbm, bias_ref),
            (lengths_hbm, lengths_ref),
        )
    ]
    query_copies = fetch(query_hbm, query_buf, 4)
    key_copies = fetch(key_hbm, key_buf, 2)
    value_copies = fetch(value_hbm, value_buf, 2)
    out_copies = fetch(out_hbm, out_buf, 1)
    router_copies = fetch(router_hbm, router_ref, 1)
    for copy in copies:
        copy.start()

    for copy in small_copies:
        copy.wait()
    normed = rms_scale(tokens_ref[...], gain_ref[...]).astype(BF16)
    parts = len(key_copies)
    part = seq_count // parts
    part_rows = row_total // parts
    row = lax.broadcasted_iota(jnp.int32, (heads * part, 1), 0)
    bias = jnp.zeros((heads * part, 1), F32)
    for h in range(heads):
        bias = jnp.where(row // part == h, bias_ref[:, h : h + 1], bias)
    low = lax.broadcasted_iota(jnp.int32, (part, 128), 1) < head_dim
    own = (
        lax.broadcasted_iota(jnp.int32, (part, part_rows), 1) // head_dim
        == lax.broadcasted_iota(jnp.int32, (part, part_rows), 0)
    )
    span = 256
    after_mask = (
        lax.broadcasted_iota(jnp.int32, (span, span), 0) > lax.broadcasted_iota(jnp.int32, (span, span), 1)
    ).astype(BF16)
    lengths = []
    for n in range(parts):
        column = jnp.zeros((part, 1), jnp.int32)
        for k in range(part):
            at = n * part + k
            column = jnp.where(row[:part] == k, lengths_ref[:, at : at + 1], column)
        lengths.append(jnp.concatenate([column] * heads, axis=0))

    queries = jnp.zeros((seq_count, head_total), F32)
    piece = width // len(query_copies)
    for n, copy in enumerate(query_copies):
        copy.wait()
        at = slice(n * piece, (n + 1) * piece)
        queries += jnp.dot(normed[:, at], query_buf[at, :], preferred_element_type=F32)
    queries = queries.astype(BF16).astype(F32)

    def spread(n):
        out = []
        for h in range(heads):
            tile = queries[n * part : (n + 1) * part, h // 2 * 128 : h // 2 * 128 + 128]
            turned = pltpu.roll(tile, head_dim, 1)
            both = jnp.where(low, tile, turned) if h % 2 == 0 else jnp.where(low, turned, tile)
            out.append(jnp.where(own, jnp.concatenate([both] * (part_rows // 128), axis=1), 0.0))
        return jnp.concatenate(out, axis=0).astype(BF16)

    def stick(scores, lengths):
        later = jnp.zeros((heads * part, 1), F32)
        out = []
        for block in reversed(range(cache_len // span)):
            score = scores[:, block * span : (block + 1) * span] * head_dim ** (-0.5) + bias
            position = lax.broadcasted_iota(jnp.int32, score.shape, 1) + block * span
            visible = position < lengths
            soft = jnp.log1p(jnp.exp(-jnp.abs(score)))
            log_keep = jnp.where(visible, -(jnp.maximum(score, 0.0) + soft), 0.0)
            high = log_keep.astype(BF16)
            rest = (log_keep - high.astype(F32)).astype(BF16)
            log_after = jnp.dot(high, after_mask, preferred_element_type=F32)
            log_after += jnp.dot(rest, after_mask, preferred_element_type=F32)
            weight = jnp.exp(jnp.minimum(score, 0.0) - soft + (log_after + later))
            out.append(jnp.where(visible, weight, 0.0).astype(BF16))
            later += jnp.sum(log_keep, axis=-1, keepdims=True)
        return jnp.concatenate(out[::-1], axis=1)

    spreads = [spread(n) for n in range(parts)]
    sticks = []
    for n, copy in enumerate(key_copies):
        copy.wait()
        keys = key_buf[n * part_rows : (n + 1) * part_rows, :]
        sticks.append(stick(jnp.dot(spreads[n], keys, preferred_element_type=F32), lengths[n]))
    heads_out = []
    for n, copy in enumerate(value_copies):
        copy.wait()
        values = value_buf[n * part_rows : (n + 1) * part_rows, :]
        read = lax.dot_general(sticks[n], values, (((1,), (1,)), ((), ())), preferred_element_type=F32)
        folded = []
        for h in range(heads):
            mine = jnp.where(own, read[h * part : (h + 1) * part], 0.0)
            tile = mine[:, :128]
            for k in range(1, part_rows // 128):
                tile += mine[:, k * 128 : (k + 1) * 128]
            folded.append(tile + pltpu.roll(tile, head_dim, 1))
        heads_out.append(
            jnp.concatenate([jnp.where(low, folded[h], folded[h + 1]) for h in range(0, heads, 2)], axis=1)
        )
    heads_out = jnp.concatenate(heads_out, axis=0).astype(BF16)
    for copy in out_copies:
        copy.wait()
    partial_ref[...] = jnp.dot(heads_out, out_buf[...], preferred_element_type=F32).astype(BF16)
    for copy in router_copies:
        copy.wait()


def call(kernel, out_shape, smem_count, inputs, limit, hbm_count=0, scratch=()):
    in_specs = [pl.BlockSpec(memory_space=pltpu.SMEM)] * smem_count
    in_specs += [pl.BlockSpec(memory_space=pltpu.VMEM)] * (len(inputs) - smem_count - hbm_count)
    in_specs += [pl.BlockSpec(memory_space=pltpu.HBM)] * hbm_count
    held = [pltpu.with_memory_space_constraint(x, pltpu.HBM) for x in inputs[len(inputs) - hbm_count :]]
    return pl.pallas_call(
        kernel,
        out_shape=out_shape,
        in_specs=in_specs,
        out_specs=jax.tree.map(lambda _: pl.BlockSpec(memory_space=pltpu.VMEM), out_shape),
        scratch_shapes=scratch,
        compiler_params=pltpu.CompilerParams(vmem_limit_bytes=limit * 1024 * 1024),
    )(*inputs[: len(inputs) - hbm_count], *held)


def rows_kernel(
    core_ref,
    line_ref,
    tokens_ref,
    own_ref,
    other_ref,
    gain_ref,
    router_ref,
    routes_ref,
    gate_ref,
    up_ref,
    down_ref,
    mix_ref,
    send_ref,
    residual_ref,
):
    first_core = core_ref[0] == 0
    lines, seq_count, _ = send_ref.shape
    half = residual_ref.shape[1]
    attn = own_ref[...].astype(F32) + other_ref[...].astype(F32)
    residual = (tokens_ref[...].astype(F32) + attn).astype(BF16)
    normed = rms_scale(residual, gain_ref[...]).astype(BF16)
    residual_ref[...] = jnp.where(first_core, residual[:, :half], residual[:, half:])
    probs = jax.nn.sigmoid(jnp.dot(normed, router_ref[...], preferred_element_type=F32))
    mix = jax.nn.sigmoid(jnp.sum(normed.astype(F32) * mix_ref[...], axis=-1, keepdims=True))
    routes = routes_ref[...]
    lane = lax.broadcasted_iota(jnp.int32, probs.shape, 1)
    picked = [
        jnp.sum(jnp.where(lane == routes[:, k : k + 1], probs, 0.0), axis=-1, keepdims=True)
        for k in range(routes.shape[1])
    ]
    total = sum(picked[1:], picked[0])
    meta_lane = lax.broadcasted_iota(jnp.int32, (seq_count, 128), 1)
    meta = jnp.zeros((seq_count, 128), F32)

    def put(meta, at, value):
        return jnp.where(meta_lane == at, value, meta)

    for k, one in enumerate(picked):
        gate = one / total * 2.5
        high = gate.astype(BF16).astype(F32)
        meta = put(meta, k, routes[:, k : k + 1].astype(F32))
        meta = put(meta, GATE_HI + k, high)
        meta = put(meta, GATE_LO + k, gate - high)
    mix_high = mix.astype(BF16).astype(F32)
    meta = put(put(meta, MIX_HI, mix_high), MIX_LO, mix - mix_high)
    parts = [ref[...].astype(F32) for ref in (gate_ref, up_ref, down_ref)]
    part = parts[0].shape[1] // lines
    row = jnp.where(first_core, normed[:, :half], normed[:, half:])
    for line in range(lines):
        block = meta
        at = line * part
        for n, values in enumerate(parts):
            tile = values[:, at // 128 * 128 : at // 128 * 128 + 128]
            to = DENSE + n * part
            moved = pltpu.roll(tile, (to - at % 128) % 128, 1)
            inside = jnp.logical_and(meta_lane >= to, meta_lane < to + part)
            block = jnp.where(inside, moved, block)
        send_ref[line, :, :half] = row
        send_ref[line, :, half:] = block.astype(BF16)


def slot_map(line, got, lines, seq_count, places, width):
    token_total = lines * seq_count
    capacity = seq_count
    shape = (places * capacity, token_total)
    meta = got[:, width - 128 :].astype(F32).T
    slot = lax.broadcasted_iota(jnp.int32, shape, 0)
    token = lax.broadcasted_iota(jnp.int32, shape, 1)
    expert = (line * places + slot // capacity).astype(F32)
    hit = jnp.zeros(shape, F32)
    gate = jnp.zeros(shape, F32)
    for k in range(6):
        same = meta[k : k + 1] == expert
        hit = jnp.where(same, 1.0, hit)
        gate = jnp.where(same, meta[GATE_HI + k : GATE_HI + k + 1] + meta[GATE_LO + k : GATE_LO + k + 1], gate)
    row = lax.broadcasted_iota(jnp.int32, (token_total, token_total), 0)
    column = lax.broadcasted_iota(jnp.int32, (token_total, token_total), 1)
    earlier = jnp.logical_and(row // seq_count == column // seq_count, row < column)
    rank = jnp.dot(hit.astype(BF16), earlier.astype(BF16), preferred_element_type=F32)
    per_source = capacity // lines
    here = jnp.logical_and(
        token // seq_count == slot % capacity // per_source,
        rank == (slot % per_source).astype(F32),
    )
    return jnp.where(here, hit, 0.0), jnp.where(here, gate * hit, 0.0)


def slots_kernel(line_ref, got_ref, send_ref):
    lines, seq_count, width = got_ref.shape
    places = send_ref.shape[0]
    half = width - 128
    capacity = seq_count
    got = got_ref[...].reshape(lines * seq_count, width)
    chosen, _ = slot_map(line_ref[0], got, lines, seq_count, places, width)
    rows = jnp.dot(chosen.astype(BF16), got[:, :half], preferred_element_type=F32)
    send_ref[:, :, :half] = rows.astype(BF16).reshape(places, capacity, half)
    group = (lax.broadcasted_iota(jnp.int32, (seq_count, 128), 1)) // 32
    for n in range(3):
        for first in range(0, lines, 4):
            tile = jnp.zeros((seq_count, 128), F32)
            for k in range(4):
                block = got[(first + k) * seq_count : (first + k + 1) * seq_count, half:].astype(F32)
                moved = pltpu.roll(block, (k * 32 - DENSE - n * 32) % 128, 1)
                tile = jnp.where(group == k, moved, tile)
            at = half + (n * lines + first) * 32
            send_ref[:, :, at : at + 128] = jnp.broadcast_to(tile.astype(BF16)[None], (places, seq_count, 128))


def dense_weights(slots_ref, half, part, line):
    lanes = 32 * 8
    at = pl.multiple_of(half + part * lanes + line // 4 * 128, 128)
    return slots_ref[:, :, pl.ds(at, 128)].reshape(-1, 128)


def lane_group(shape):
    return lax.broadcasted_iota(jnp.int32, shape, 1) // 32


def half_products(side, slots_ref, width, gate_ref, up_ref):
    half = width // 2
    mine = pl.ds(pl.multiple_of(side * half, half), half)
    values = slots_ref[:, :, :half].reshape(-1, half)
    return tuple(jnp.dot(values, ref[mine, :], preferred_element_type=F32) for ref in (gate_ref, up_ref))


def dense_share(core, slots_ref, line_own_ref, line_other_ref):
    half = line_own_ref.shape[2] - 128
    block = half // 4
    group = lane_group((line_own_ref.shape[0] * line_own_ref.shape[1], 128))
    sums = []
    for part in range(2):
        total = jnp.zeros(group.shape, F32)
        for side, line_ref in ((core, line_own_ref), (1 - core, line_other_ref)):
            rows = line_ref[:, :, :half].reshape(-1, half)
            weights = dense_weights(slots_ref, half, part, side * 4)
            for k in range(4):
                product = jnp.dot(rows[:, k * block : (k + 1) * block], weights, preferred_element_type=F32)
                total += jnp.where(group == k, product, 0.0)
        total += pltpu.roll(total, 64, 1)
        sums.append(total + pltpu.roll(total, 32, 1))
    hidden = (jax.nn.silu(sums[0]) * sums[1]).astype(BF16).astype(F32)
    weights = dense_weights(slots_ref, half, 2, core * 4)
    return [
        lax.dot_general(
            jnp.where(group == k, hidden, 0.0).astype(BF16),
            weights,
            (((1,), (1,)), ((), ())),
            preferred_element_type=F32,
        )
        for k in range(4)
    ]


def own_kernel(
    core_ref,
    line_ref,
    slots_ref,
    got_ref,
    gate_ref,
    up_ref,
    tokens_ref,
    gain_ref,
    key_ref,
    value_ref,
    gate_out,
    up_out,
    keys_ref,
    values_ref,
    combine_ref,
):
    core = core_ref[0]
    gate_out[...], up_out[...] = half_products(core, slots_ref, gate_ref.shape[0], gate_ref, up_ref)
    normed = rms_scale(tokens_ref[...], gain_ref[...]).astype(BF16)
    for weight_ref, target_ref in ((key_ref, keys_ref), (value_ref, values_ref)):
        target_ref[...] = lax.dot_general(
            normed, weight_ref[...], (((1,), (1,)), ((), ())), preferred_element_type=F32
        ).astype(BF16)
    lines, seq_count, width = got_ref.shape
    got = got_ref[...].reshape(lines * seq_count, width)
    gates = slot_map(line_ref[0], got, lines, seq_count, slots_ref.shape[0], width)[1].T
    high = gates.astype(BF16)
    slot_total = gates.shape[1]
    combine_ref[:, :slot_total] = high
    combine_ref[:, slot_total:] = (gates - high.astype(F32)).astype(BF16)


def down_product(side, hidden, down_ref):
    half = down_ref.shape[1] // 2
    mine = pl.ds(pl.multiple_of(side * half, half), half)
    return jnp.dot(hidden, down_ref[:, mine], preferred_element_type=F32).astype(BF16)


def other_kernel(
    core_ref, gate_sum, up_sum, other_ref, line_other_ref, gate_ref, up_ref, down_ref, send_ref, hidden_ref
):
    del line_other_ref
    side = 1 - core_ref[0]
    gate, up = half_products(side, other_ref, gate_ref.shape[0], gate_ref, up_ref)
    hidden = (jax.nn.silu(gate_sum[...] + gate) * (up_sum[...] + up)).astype(BF16)
    hidden_ref[...] = hidden
    send_ref[...] = down_product(side, hidden, down_ref)


def keep_kernel(
    core_ref, hidden_ref, down_ref, own_ref, other_ref, line_own_ref, line_other_ref, keep_ref, dense_out
):
    core = core_ref[0]
    keep_ref[...] = down_product(core, hidden_ref[...], down_ref)
    block = dense_out.shape[1] // 4
    shares = [dense_share(core, ref, line_own_ref, line_other_ref) for ref in (own_ref, other_ref)]
    for k, (own, other) in enumerate(zip(*shares, strict=True)):
        dense_out[:, k * block : (k + 1) * block] = own + other


def combine_kernel(back_ref, combine_ref, line_ref, dense_ref, send_ref):
    lines, seq_count, half = send_ref.shape
    token_total = lines * seq_count
    slot_total = back_ref.shape[0] * back_ref.shape[1]
    back = back_ref[...].reshape(slot_total, half)
    routed = jnp.dot(combine_ref[:, :slot_total], back, preferred_element_type=F32)
    routed += jnp.dot(combine_ref[:, slot_total:], back, preferred_element_type=F32)
    meta = line_ref[...].reshape(token_total, line_ref.shape[2])[:, half:].astype(F32)
    mix = meta[:, MIX_HI : MIX_HI + 1] + meta[:, MIX_LO : MIX_LO + 1]
    send_ref[...] = (routed + mix * dense_ref[...]).astype(BF16).reshape(lines, seq_count, half)


def finish_kernel(residual_ref, parts_ref, out_ref):
    total = parts_ref[0].astype(F32)
    for n in range(1, parts_ref.shape[0]):
        total += parts_ref[n].astype(F32)
    out_ref[...] = (residual_ref[...].astype(F32) + total).astype(BF16)


def shards(
    tokens,
    lengths,
    attn_gain,
    w_query,
    w_key,
    w_value,
    head_bias,
    key_cache,
    value_cache,
    w_attn_out,
    ffn_gain,
    w_router,
    routes,
    w_dense_gate,
    w_dense_up,
    w_dense_down,
    dense_mix,
    w_expert_gate,
    w_expert_up,
    w_expert_down,
):
    seq_count, width = tokens.shape
    half = width // 2
    lines = lax.axis_size(LINE)
    places = lax.axis_size(PLANE)
    slot_total = places * seq_count
    token_total = lines * seq_count
    core = lax.axis_index("tp").astype(jnp.int32).reshape(1)
    line = lax.axis_index(LINE).astype(jnp.int32).reshape(1)
    cache_rows = seq_count * key_cache.shape[2]
    cache_len = key_cache.shape[3]
    attn_own, router = call(
        attend_kernel,
        (jax.ShapeDtypeStruct((seq_count, width), BF16), jax.ShapeDtypeStruct(w_router.shape, BF16)),
        0,
        (
            head_bias.reshape(1, -1),
            lengths.reshape(1, seq_count),
            tokens,
            attn_gain.reshape(1, width),
            w_query,
            key_cache.reshape(cache_rows, cache_len),
            value_cache.reshape(cache_rows, cache_len),
            w_attn_out,
            w_router,
        ),
        24,
        hbm_count=9,
        scratch=(
            pltpu.VMEM((1, head_bias.shape[0]), F32),
            pltpu.VMEM((1, seq_count), jnp.int32),
            pltpu.VMEM(tokens.shape, BF16),
            pltpu.VMEM((1, width), F32),
            pltpu.VMEM(w_query.shape, BF16),
            pltpu.VMEM((cache_rows, cache_len), BF16),
            pltpu.VMEM((cache_rows, cache_len), BF16),
            pltpu.VMEM(w_attn_out.shape, BF16),
            pltpu.SemaphoreType.DMA((14,)),
        ),
    )
    attn_other = lax.ppermute(attn_own, "tp", SWAP)
    line_send, residual = call(
        rows_kernel,
        (
            jax.ShapeDtypeStruct((lines, seq_count, half + 128), BF16),
            jax.ShapeDtypeStruct((seq_count, half), BF16),
        ),
        2,
        (
            core,
            line,
            tokens,
            attn_own,
            attn_other,
            ffn_gain.reshape(1, width),
            router,
            routes,
            w_dense_gate,
            w_dense_up,
            w_dense_down.T,
            dense_mix.reshape(1, width),
        ),
        8,
    )
    line_own = lax.all_to_all(line_send, LINE, 0, 0, tiled=True)
    line_other = lax.ppermute(line_own, "tp", SWAP)
    slot_send = call(
        slots_kernel,
        jax.ShapeDtypeStruct((places, seq_count, half + 96 * lines), BF16),
        1,
        (line, line_own),
        8,
    )
    slot_own = lax.all_to_all(slot_send, PLANE, 0, 0, tiled=True)
    slot_other = lax.ppermute(slot_own, "tp", SWAP)
    weights = (w_expert_gate[0], w_expert_up[0])
    hidden_shape = (slot_total, w_expert_gate.shape[2])
    hidden_shape = (slot_total, w_expert_gate.shape[2])
    new_shape = jax.ShapeDtypeStruct((seq_count, w_key.shape[1]), BF16)
    dense_shape = jax.ShapeDtypeStruct((token_total, half), F32)
    gate_sum, up_sum, new_keys, new_values, combine = call(
        own_kernel,
        (
            *(jax.ShapeDtypeStruct(hidden_shape, F32),) * 2,
            new_shape,
            new_shape,
            jax.ShapeDtypeStruct((token_total, 2 * slot_total), BF16),
        ),
        2,
        (core, line, slot_own, line_own, *weights, tokens, attn_gain.reshape(1, width), w_key.T, w_value.T),
        8,
    )
    result_shape = jax.ShapeDtypeStruct((slot_total, half), BF16)
    send, hidden = call(
        other_kernel,
        (result_shape, jax.ShapeDtypeStruct(hidden_shape, BF16)),
        1,
        (core, gate_sum, up_sum, slot_other, line_other, *weights, w_expert_down[0]),
        12,
    )
    got = lax.ppermute(send, "tp", SWAP)
    keep, dense = call(
        keep_kernel,
        (result_shape, dense_shape),
        1,
        (core, hidden, w_expert_down[0], slot_own, slot_other, line_own, line_other),
        12,
    )
    results = (keep.astype(F32) + got.astype(F32)).astype(BF16)
    back = lax.all_to_all(results.reshape(places, seq_count, half), PLANE, 0, 0, tiled=True)
    partial = call(
        combine_kernel,
        jax.ShapeDtypeStruct((lines, seq_count, half), BF16),
        0,
        (back, combine, line_own, dense),
        8,
    )
    parts = lax.all_to_all(partial, LINE, 0, 0, tiled=True)
    layer_out = call(finish_kernel, jax.ShapeDtypeStruct((seq_count, half), BF16), 0, (residual, parts), 8)
    return (layer_out, new_keys, new_values)


def solution(mesh):
    finer = Mesh(mesh.devices.reshape(8, 4, 4, mesh.shape["tp"]), ("ep_0", "ep_1", "ep_2", "tp"))
    placed = (
        P(EP, None),
        P(EP),
        P(),
        P(None, "tp"),
        P(None, "tp"),
        P(None, "tp"),
        P("tp"),
        P(EP, "tp", None, None),
        P(EP, "tp", None, None),
        P("tp", None),
        P(),
        P(),
        P(EP, None),
        P(EP, "tp"),
        P(EP, "tp"),
        P("tp", EP),
        P(),
        P(EP, None, "tp"),
        P(EP, None, "tp"),
        P(EP, "tp", None),
    )
    return jax.shard_map(
        shards,
        mesh=finer,
        in_specs=placed,
        out_specs=(P(EP, "tp"), P(EP, "tp"), P(EP, "tp")),
        check_vma=False,
    )
```
